32 devices in a mesh: ep: 8 (over z, core), tp: 4 (over y, x).
Axes of the slice: x: 2, y: 2, z: 4, core: 2. Of those that a mesh axis runs over, the one named last changes fastest.
Arguments:
- q_latent: bfloat16 [1536, 512], P('ep'), may hold values from -6 to 6
- kv_latent: bfloat16 [1536, 256], P('ep'), may hold values from -6 to 6
- rope_key: bfloat16 [1536, 64], P('ep'), may hold values from -900 to 900
- q_gain: float32 [512], replicated, may hold values from 0.1 to 1.9
- kv_gain: float32 [256], replicated, may hold values from 0.1 to 1.9
- w_query: bfloat16 [512, 3072], P(None, 'tp'), may hold values from -0.25 to 0.25
- w_key: bfloat16 [256, 2048], P(None, 'tp'), may hold values from -0.375 to 0.375
- w_value: bfloat16 [256, 2048], P(None, 'tp'), may hold values from -0.375 to 0.375
- w_mix_out: bfloat16 [2048, 2048], P('tp'), may hold values from -0.125 to 0.125
- expert_in: bfloat16 [1024, 2048], P('ep'), may hold values from -6 to 6
- norm_gain: float32 [2048], replicated, may hold values from 0.1 to 1.9
- routes: int32 [1024, 2], P('ep'), may hold values from 0 to 7, all different within a row; in each aligned block of 128 rows (0 to 127, 128 to 255, ...) at most 64 rows name the same one
- route_scores: float32 [1024, 2], P('ep'), may hold values from 0.05 to 1
- w_gate: bfloat16 [8, 2048, 4096], P('ep', None, 'tp'), may hold values from -0.125 to 0.125
- w_up: bfloat16 [8, 2048, 4096], P('ep', None, 'tp'), may hold values from -0.125 to 0.125
- w_down: bfloat16 [8, 4096, 2048], P('ep', 'tp'), may hold values from -0.125 to 0.125
Outputs:
- mixed: bfloat16 [1536, 2048], P(('ep', 'tp'))
- expert_out: bfloat16 [1024, 2048], P('ep', 'tp')
The draws below stay inside these ranges and needn't reach their ends.
Inputs may be any that keep to these rules, and one draw needn't show every extreme that they name: `routes`: each row names 2 different experts; in the rows of one index of ep no expert is named by more than 64 rows, a bound that some block reaches.
All inputs are finite; a program needn't handle non-finite values.
Results may differ from the reference program's by a relative error of at most 0.03.
The reference program's roundings to bfloat16 on the way count: a program that leaves them out, or rounds other values in their place, can miss the bound.
Values may be sent and summed in bfloat16 or wider, within the bound.
A program may use at most 64 MiB of HBM per device.

```python
import math
import jax
import jax.numpy as jnp
import numpy as np
from jax import lax

D = 2048
HEADS = 16
QR = 512
KVR = 256
NOPE = 128
ROPE = 64
VDIM = 128
FF = 4096
TOP = 2
TOKA = 192
TOKB = 128
EXPERTS = 8
CAP = 64
N_EP = 8
N_TP = 4


def draw_rope_key(key, part):
    length = TOKA * N_EP
    base = jnp.clip(jax.random.normal(jax.random.fold_in(key, 11), (length, ROPE), jnp.float32), -6.0, 6.0)
    return base.astype(jnp.bfloat16)


def strengthened(array, rng, source, target, shards_of, factor):
    def block_of(axis_at):
        return (jnp.arange(array.shape[axis_at]) // (array.shape[axis_at] // shards_of)).reshape((-1,) + (1,) * (array.ndim - 1 - axis_at))

    first = jax.random.permutation(rng, shards_of)[block_of(target)]
    far = (block_of(target) + shards_of // 2) % shards_of
    return jnp.where((block_of(source) == first) | (block_of(source) == far), factor * array, array)


def level_of(key, extent, cuts, least, top_value):
    level, own = 1.0, jax.random.fold_in(key, 6)
    for axis_at, shards_of in cuts:
        heights = jnp.exp(jax.random.uniform(jax.random.fold_in(own, axis_at), (shards_of,), jnp.float32, least / len(cuts), top_value / len(cuts)))
        level = level * jnp.repeat(heights, extent[axis_at] // shards_of).reshape([-1 if axis == axis_at else 1 for axis in range(len(extent))])
    return level


def assign_block(key, own, number, rows, count, top, bound, skew):
    ranking = jax.random.permutation(key, count)
    heavy_load, usual = load_shares(count, rows * top, bound, skew, True), load_shares(count, rows * top, bound, skew, False)
    places = jnp.arange(count)

    def named(tallies, offset_by):
        used = int((tallies > 0).sum())
        fixed = max(1, used // 4)
        moved = fixed + (places - fixed + offset_by * (used - fixed)) % max(1, count - fixed)
        return jnp.zeros((count,), jnp.int32).at[ranking[jnp.where(places < fixed, places, moved)]].set(jnp.asarray(tallies, jnp.int32))

    tallies = jnp.where(number % 4 == 0, named(heavy_load, number // 4), named(usual, number - number // 4 - 1))
    mixed = jax.random.permutation(jax.random.fold_in(own, 3), count)
    source_of, taker = mixed[0:count // 2 * 2:2], mixed[1:count // 2 * 2:2]
    room = jnp.minimum(tallies[source_of] - 1, bound - tallies[taker]) // 2
    room = jnp.where((source_of == ranking[0]) | (taker == ranking[0]) | (tallies[taker] == 0), 0, jnp.maximum(room, 0))
    moved = jax.random.randint(jax.random.fold_in(own, 4), (count // 2,), 0, 1 << 20) % (room + 1)
    tallies = tallies.at[source_of].add(-moved).at[taker].add(moved)
    labels = jnp.searchsorted(jnp.cumsum(tallies), jnp.arange(rows * top), side="right").astype(jnp.int32)
    listing = labels.reshape(top, rows).T
    listing = listing[jax.random.permutation(jax.random.fold_in(own, 1), rows)]
    offset_by = jax.random.randint(jax.random.fold_in(own, 2), (rows, 1), 0, top)
    return jnp.take_along_axis(listing, (jnp.arange(top)[None, :] + offset_by) % top, axis=1)


def load_shares(amount, total, limit, lean, full):
    portions = [(1 << 20) // math.isqrt(grade ** lean) + 1 for grade in range(1, amount + 1)]
    largest = limit if full else min(limit, max(-(-total // amount), total * portions[0] // sum(portions)))
    least = 1 if total - largest >= amount - 1 else 0
    counts, surplus = [largest] + [least] * (amount - 1), total - largest - least * (amount - 1)
    while surplus > 0:
        movable = [i for i in range(1, amount) if counts[i] < largest] or [i for i in range(1, amount) if counts[i] < limit]
        pool, budget = sum([portions[i] for i in movable]), surplus
        for i in movable:
            addition = min(limit - counts[i], max(1, budget * portions[i] // pool), surplus)
            counts[i] = counts[i] + addition
            surplus = surplus - addition
    return np.array(counts)


def gaussian(own_key, dims, scale, limit, shards=(), held_as=jnp.bfloat16):
    entries = jax.random.normal(own_key, dims, jnp.float32) * scale
    if len(shards) > 0:
        entries = level_of(own_key, dims, shards, -0.22, 0.18) * entries
    return jnp.clip(entries, min=-limit, max=limit).astype(held_as)


def heavy_noise(key, shape, width, most, shards, heavy, kind=jnp.bfloat16):
    result = width * jax.random.normal(key, shape, jnp.float32)
    if shards:
        result = result * level_of(key, shape, shards, -0.22, 0.18)
    return jnp.clip(strengthened(result, jax.random.fold_in(key, 3), *heavy), -most, most).astype(kind)


def setup_inputs(seed: int = 0) -> dict:
    splits = jax.random.split(jax.random.key(seed), 17)
    q_latent = gaussian(splits[0], (TOKA * N_EP, QR), 1.0, 6.0, ((0, 8),))
    kv_latent = gaussian(splits[1], (TOKA * N_EP, KVR), 1.0, 6.0, ((0, 8),))
    rope_key = draw_rope_key(jax.random.fold_in(splits[16], 71), 0)
    q_gain = jnp.clip(1.0 + 0.18 * jax.random.normal(splits[3], (QR,), jnp.float32), 0.1, 1.9)
    kv_gain = jnp.clip(1.0 + 0.18 * jax.random.normal(splits[4], (KVR,), jnp.float32), 0.1, 1.9)
    w_query = gaussian(splits[5], (QR, HEADS * (NOPE + ROPE)), QR ** -0.5, 0.25, ((1, 4),))
    w_key = gaussian(splits[6], (KVR, HEADS * NOPE), KVR ** -0.5, 0.375, ((1, 4),))
    w_value = gaussian(splits[7], (KVR, HEADS * VDIM), KVR ** -0.5, 0.375, ((1, 4),))
    w_mix_out = gaussian(splits[8], (HEADS * VDIM, D), (HEADS * VDIM) ** -0.5, 0.125, ((0, 4),))
    expert_in = gaussian(splits[9], (TOKB * N_EP, D), 1.0, 6.0, ((0, 8),))
    norm_gain = jnp.clip(1.0 + 0.18 * jax.random.normal(splits[10], (D,), jnp.float32), 0.1, 1.9)
    routes_keys = jax.random.split(jax.random.fold_in(splits[11], 1), (TOKB * N_EP) // TOKB)
    routes_turns = jax.random.permutation(jax.random.fold_in(splits[11], 3), (TOKB * N_EP) // TOKB)
    routes = jax.vmap(lambda own, number: assign_block(jax.random.fold_in(splits[11], 2), own, number, TOKB, EXPERTS, TOP, CAP, 2))(routes_keys, routes_turns).reshape((TOKB * N_EP, TOP))
    route_scores = jnp.clip(jnp.exp(math.log(1.0) - 2.9957323 * jax.random.uniform(splits[12], (TOKB * N_EP, TOP), jnp.float32) ** level_of(splits[12], (TOKB * N_EP, TOP), ((0, 8),), -0.2, 0.2)), 0.05, 1.0)
    w_gate = gaussian(splits[13], (EXPERTS, D, FF), D ** -0.5, 0.125, ((0, 8), (2, 4)))
    w_up = gaussian(splits[14], (EXPERTS, D, FF), D ** -0.5, 0.125, ((0, 8), (2, 4)))
    w_down = heavy_noise(splits[15], (EXPERTS, FF, D), FF ** -0.5, 0.125, ((0, 8), (1, 4)), (1, 2, 4, 2.0))
    return {"q_latent": q_latent, "kv_latent": kv_latent, "rope_key": rope_key, "q_gain": q_gain, "kv_gain": kv_gain, "w_query": w_query, "w_key": w_key, "w_value": w_value, "w_mix_out": w_mix_out, "expert_in": expert_in, "norm_gain": norm_gain, "routes": routes, "route_scores": route_scores, "w_gate": w_gate, "w_up": w_up, "w_down": w_down}


eps_norm = 1e-05
rope_base = 10000.0

def rms_scale(values, gain):
    wide = values.astype(jnp.float32)
    return wide * lax.rsqrt(lax.optimization_barrier(jnp.mean(wide * wide, -1, keepdims=True)) + eps_norm) * gain

def rotate(values, cosine, sine):
    first, second = jnp.split(values, 2, axis=-1)
    return jnp.concatenate([first * cosine - second * sine, first * sine + second * cosine], -1)

def angles(positions):
    inverse = rope_base ** (-jnp.arange(0, ROPE, 2).astype(jnp.float32) / ROPE)
    phase = positions[:, None] * inverse[None, :]
    return (jnp.cos(phase), jnp.sin(phase))

def grouped_sum(left, right, groups):
    length = left.shape[0]
    inner = left.shape[1] // groups
    left_groups = jnp.transpose(left.reshape(length, groups, inner), (1, 0, 2))
    right_groups = right.reshape(groups, inner, right.shape[1])

    def add_group(total, pair):
        part = jnp.dot(pair[0], pair[1], preferred_element_type=jnp.float32).astype(jnp.bfloat16)
        part = lax.optimization_barrier(part)
        return (total + part.astype(jnp.float32), None)
    start_total = jnp.zeros((length, right.shape[1]), jnp.float32)
    total, unused = lax.scan(add_group, start_total, (left_groups, right_groups))
    return total.astype(jnp.bfloat16)

def reference(q_latent, kv_latent, rope_key, q_gain, kv_gain, w_query, w_key, w_value, w_mix_out, expert_in, norm_gain, routes, route_scores, w_gate, w_up, w_down):
    length = q_latent.shape[0]
    positions = jnp.arange(length, dtype=jnp.int32).astype(jnp.float32)
    cosine, sine = angles(positions)
    q_normed = rms_scale(q_latent, q_gain).astype(jnp.bfloat16)
    kv_normed = rms_scale(kv_latent, kv_gain).astype(jnp.bfloat16)
    query = jnp.dot(q_normed, w_query, preferred_element_type=jnp.float32).astype(jnp.bfloat16)
    query = query.reshape(length, HEADS, NOPE + ROPE)
    q_pass = query[:, :, :NOPE]
    q_rot = rotate(query[:, :, NOPE:].astype(jnp.float32), cosine[:, None, :], sine[:, None, :]).astype(jnp.bfloat16)
    k_rot = rotate(rope_key.astype(jnp.float32), cosine, sine).astype(jnp.bfloat16)
    keys = jnp.dot(kv_normed, w_key, preferred_element_type=jnp.float32).astype(jnp.bfloat16).reshape(length, HEADS, NOPE)
    values = jnp.dot(kv_normed, w_value, preferred_element_type=jnp.float32).astype(jnp.bfloat16).reshape(length, HEADS, VDIM)
    factor = (NOPE + ROPE) ** (-0.5)

    def attend_head(inputs):
        pass_head, rot_head, key_head, value_head = inputs
        scores = jnp.dot(pass_head, key_head.T, preferred_element_type=jnp.float32)
        scores = (scores + jnp.dot(rot_head, k_rot.T, preferred_element_type=jnp.float32)) * factor
        peak = lax.optimization_barrier(jnp.max(scores, -1, keepdims=True))
        weights = jnp.exp(scores - peak)
        total = lax.optimization_barrier(jnp.sum(weights, -1, keepdims=True))
        summed = jnp.dot(weights.astype(jnp.bfloat16), value_head, preferred_element_type=jnp.float32)
        return (summed / total).astype(jnp.bfloat16)
    per_head = lax.map(attend_head, (jnp.transpose(q_pass, (1, 0, 2)), jnp.transpose(q_rot, (1, 0, 2)), jnp.transpose(keys, (1, 0, 2)), jnp.transpose(values, (1, 0, 2))))
    attended = jnp.transpose(per_head, (1, 0, 2)).reshape(length, HEADS * VDIM)
    mixed = grouped_sum(attended, w_mix_out, N_TP)
    token_total = expert_in.shape[0]
    wide = expert_in.astype(jnp.float32)
    centered = wide - lax.optimization_barrier(jnp.mean(wide, -1, keepdims=True))
    normed = (centered * lax.rsqrt(lax.optimization_barrier(jnp.mean(centered * centered, -1, keepdims=True)) + eps_norm) * norm_gain).astype(jnp.bfloat16)
    shares = route_scores / lax.optimization_barrier(jnp.sum(route_scores, -1, keepdims=True))
    flat_expert = routes.reshape(-1).astype(jnp.int32)
    copies = flat_expert.shape[0]
    group_of = (jnp.arange(copies, dtype=jnp.int32) // (TOKB * TOP)).astype(jnp.int32)
    onehot = (flat_expert[:, None] == jnp.arange(EXPERTS, dtype=jnp.int32)[None, :]).astype(jnp.int32)
    within = onehot.reshape(N_EP, TOKB * TOP, EXPERTS)
    before = (jnp.cumsum(within, 1) - within).reshape(copies, EXPERTS)
    rank = lax.optimization_barrier(jnp.sum(before * onehot, 1)).astype(jnp.int32)
    slot = (group_of * CAP + rank).astype(jnp.int32)
    source = (jnp.arange(copies, dtype=jnp.int32) // TOP).astype(jnp.int32)
    table = jnp.full((EXPERTS, N_EP * CAP), token_total, jnp.int32).at[flat_expert, slot].set(source)
    padded = jnp.concatenate([normed, jnp.zeros((1, D), jnp.bfloat16)], 0)

    def one_expert(inputs):
        index, gate_weight, up_weight, down_weight = inputs
        arrived = padded[index]
        gate = jnp.dot(arrived, gate_weight, preferred_element_type=jnp.float32)
        up = jnp.dot(arrived, up_weight, preferred_element_type=jnp.float32)
        hidden = (jax.nn.silu(gate) * up).astype(jnp.bfloat16)
        return grouped_sum(hidden, down_weight, N_TP)
    results = lax.map(one_expert, (table, w_gate, w_up, w_down))
    picked = results[flat_expert, slot].astype(jnp.float32).reshape(token_total, TOP, D)
    expert_out = lax.optimization_barrier(jnp.sum(picked * shares[:, :, None], 1)).astype(jnp.bfloat16)
    return (mixed, expert_out)
```

```python
import functools

import jax
import jax.numpy as jnp
from jax import lax
from jax.experimental import pallas as pl
from jax.experimental.pallas import tpu as pltpu
from jax.sharding import PartitionSpec as P

NOPE = 128
ROPE = 64
VDIM = 128

eps_norm = 1e-05
rope_base = 10000.0

MESH = pl.DeviceIdType.MESH
F32 = jnp.float32
BF16 = jnp.bfloat16


def remote(src, dst, send, recv, ep, tp):
    return pltpu.make_async_remote_copy(
        src_ref=src, dst_ref=dst, send_sem=send, recv_sem=recv, device_id=(ep, tp), device_id_type=MESH
    )


def dot(left, right):
    return jnp.dot(left, right, preferred_element_type=F32)


def rms_scale(values, gain):
    wide = values.astype(F32)
    return wide * lax.rsqrt(jnp.mean(wide * wide, -1, keepdims=True) + eps_norm) * gain


def rotate(values, table, copies):
    source = lax.broadcasted_iota(jnp.int32, (ROPE, 256), 0)
    lane = lax.broadcasted_iota(jnp.int32, (ROPE, 256), 1)
    same = (lane < ROPE) & (lane == source)
    turned = (lane >= 128) & (lane < 128 + ROPE) & (source == (lane - 128 + ROPE // 2) % ROPE)
    spread = jnp.where(same | turned, 1.0, 0.0).astype(BF16)
    wide = dot(values, spread)
    cosine, sine = table[:, :128], table[:, 128:]
    if copies > 1:
        cosine = jnp.concatenate([cosine] * copies, 0)
        sine = jnp.concatenate([sine] * copies, 0)
    return (wide[:, :128] * cosine + wide[:, 128:] * sine).astype(BF16)


def layer_kernel(
    sizes,
    q_lat, kv_lat, rope_key, q_gain, kv_gain, table, table_q, expert_in, norm_gain, routes, scores,
    w_query, w_key, w_value, w_mix, w_gate, w_up, w_down,
    mixed, expert_out,
    v_query, v_key, v_value, v_mix, v_gate, v_up, v_down,
    latent, kcat, vals, qcat, attended, mix_part, mix_landed,
    normed, place, facts, send_rows, twin_rows, rows, hidden, part_rows, landed, reduced, comb,
    w_sem, kz_send, kz_recv, kt_send, kt_recv, kc_send, kc_recv, ko_send, ko_recv,
    dz_send, dz_recv, dt_send, dt_recv, do_send, do_recv,
    p_send, p_recv, r_send, r_recv, m_send, m_recv,
):
    ep_size, tp_size, slots, choose, heads, split = sizes
    levels = ep_size // 2
    me = lax.axis_index("ep")
    part = lax.axis_index("tp")
    level, core = me // 2, me % 2
    twin = level * 2 + 1 - core
    tokens, width = expert_in.shape
    features = width // tp_size
    rank = kv_lat.shape[1]
    queries = q_lat.shape[0]
    waits = []

    def peer(k):
        return lax.rem(part + k, tp_size)

    def columns(index):
        return pl.ds(pl.multiple_of(index * features, features), features)

    def start(copy):
        copy.start()
        waits.append(copy)

    barrier = pltpu.get_barrier_semaphore()
    for d in range(1, ep_size):
        pl.semaphore_signal(
            barrier, inc=1, device_id=(lax.rem(me + d, ep_size), part), device_id_type=MESH
        )
    for k in range(1, tp_size):
        pl.semaphore_signal(barrier, inc=1, device_id=(me, peer(k)), device_id_type=MESH)
    loads = [
        pltpu.make_async_copy(src, dst, w_sem.at[i])
        for i, (src, dst) in enumerate((
            (w_query, v_query), (w_key, v_key), (w_value, v_value), (w_gate, v_gate),
            (w_up, v_up), (w_down, v_down), (w_mix, v_mix),
        ))
    ]
    for load in loads:
        load.start()

    kv_normed = rms_scale(kv_lat[...], kv_gain[...]).astype(BF16)
    key_turned = rotate(rope_key[...], table[...], 1)
    packed = jnp.concatenate([kv_normed, key_turned], 1)
    latent[me] = packed.reshape(latent.shape[1:])

    named = routes[...]
    experts = max(8, ep_size)
    expert = lax.broadcasted_iota(jnp.int32, (experts, tokens), 0)
    member = [expert == named[k : k + 1, :] for k in range(choose)]
    any_member = member[0]
    for k in range(1, choose):
        any_member = any_member | member[k]
    earlier = lax.broadcasted_iota(jnp.int32, (tokens, tokens), 0) < lax.broadcasted_iota(
        jnp.int32, (tokens, tokens), 1
    )
    before = dot(
        jnp.where(any_member, 1.0, 0.0).astype(BF16), jnp.where(earlier, 1.0, 0.0).astype(BF16)
    )
    spot = before + (expert * slots).astype(F32)
    targets = [
        jnp.sum(jnp.where(member[k], spot, 0.0), 0, keepdims=True) for k in range(choose)
    ]
    score = scores[...]
    shares = score / jnp.sum(score, 0, keepdims=True)
    known = jnp.concatenate(targets + [shares], 0)
    known = jnp.concatenate([known, jnp.zeros((128 - 2 * choose, tokens), F32)], 0)
    facts[...] = jnp.transpose(known)
    seat = lax.broadcasted_iota(jnp.int32, (ep_size * slots, tokens), 0).astype(F32)
    chosen = seat == targets[0]
    for k in range(1, choose):
        chosen = chosen | (seat == targets[k])
    place[...] = jnp.where(chosen, 1.0, 0.0).astype(BF16)

    wide = expert_in[...].astype(F32)
    centered = wide - jnp.mean(wide, -1, keepdims=True)
    normed[...] = (
        centered
        * lax.rsqrt(jnp.mean(centered * centered, -1, keepdims=True) + eps_norm)
        * norm_gain[...]
    ).astype(BF16)

    def seats(index):
        return place[pl.ds(pl.multiple_of(index * slots, slots), slots), :]

    send_rows[...] = dot(place[...], normed[:, columns(part)]).astype(BF16).reshape(send_rows.shape)
    twin_rows[...] = dot(seats(twin), normed[...]).astype(BF16)
    rows[me] = dot(seats(me), normed[...]).astype(BF16)

    pl.semaphore_wait(barrier, ep_size + tp_size - 2)

    chunk = part if split > 1 else 0
    for d in range(1, levels):
        target = lax.rem(level + d, levels) * 2 + core
        start(remote(
            latent.at[me, chunk], latent.at[me, chunk], kz_send.at[d], kz_recv.at[d], target, part
        ))
    start(remote(latent.at[me], latent.at[me], ko_send.at[0], ko_recv.at[0], twin, part))
    start(remote(twin_rows, rows.at[me], do_send.at[0], do_recv.at[0], twin, part))
    for d in range(1, levels):
        for c in range(2):
            target = lax.rem(level + d, levels) * 2 + c
            start(remote(
                send_rows.at[target], rows.at[me, :, columns(part)],
                dz_send.at[d, c], dz_recv.at[d, core], target, part,
            ))

    def behind(d, c):
        return lax.rem(level - d + levels, levels) * 2 + c

    loads[0].wait()
    q_normed = rms_scale(q_lat[...], q_gain[...]).astype(BF16)
    query = dot(q_normed, v_query[...])
    for h in range(heads):
        base = h * (NOPE + ROPE)
        qcat[h, :, :NOPE] = query[:, base : base + NOPE].astype(BF16)
        turn = query[:, base + NOPE : base + NOPE + ROPE].astype(BF16)
        qcat[h, :, NOPE:] = rotate(turn, table_q[...], 1)

    def pass_latents(d):
        here = latent.at[behind(d, core), chunk]
        remote(here, here, kz_send.at[d], kz_recv.at[d], twin, part).wait_recv()
        if split > 1:
            for k in range(1, tp_size):
                start(remote(here, here, kt_send.at[d, k], kt_recv.at[d, k], me, peer(k)))
        start(remote(here, here, kc_send.at[d, 0], kc_recv.at[d, 0], twin, part))

    def pass_latents_on(d):
        if split > 1:
            for k in range(1, tp_size):
                here = latent.at[behind(d, core), peer(tp_size - k)]
                remote(here, here, kt_send.at[d, k], kt_recv.at[d, k], twin, part).wait_recv()
                start(remote(here, here, kc_send.at[d, k], kc_recv.at[d, k], twin, part))

    def wait_latents(d):
        for k in range(tp_size if split > 1 else 1):
            index = peer(tp_size - k) if split > 1 else 0
            here = latent.at[behind(d, 1 - core), index]
            remote(here, here, kc_send.at[d, k], kc_recv.at[d, k], twin, part).wait_recv()

    def pass_rows(d):
        for c in range(2):
            here = rows.at[behind(d, c), :, columns(part)]
            remote(here, here, dz_send.at[d, c], dz_recv.at[d, c], twin, part).wait_recv()
            for k in range(1, tp_size):
                start(remote(here, here, dt_send.at[d, c, k], dt_recv.at[d, c, k], me, peer(k)))

    def wait_rows(d):
        if d == 0:
            here = rows.at[twin]
            remote(here, here, do_send.at[0], do_recv.at[0], twin, part).wait_recv()
            return
        for c in range(2):
            for k in range(1, tp_size):
                here = rows.at[behind(d, c), :, columns(peer(tp_size - k))]
                remote(here, here, dt_send.at[d, c, k], dt_recv.at[d, c, k], twin, part).wait_recv()

    block = min(256, v_gate.shape[1])

    def run_expert(d):
        first = lax.rem(level - d + levels, levels) * 2
        wait_rows(d)
        arrived = rows[pl.ds(first, 2)].reshape(2 * slots, width)
        for j in range(v_gate.shape[1] // block):
            units = slice(j * block, (j + 1) * block)
            gate = dot(arrived, v_gate[:, units])
            up = dot(arrived, v_up[:, units])
            hidden[:, units] = (gate / (1.0 + jnp.exp(-gate)) * up).astype(BF16)
        for n in range(tp_size):
            result = dot(hidden[...], v_down[:, n * features : (n + 1) * features]).astype(BF16)
            part_rows[pl.ds(first, 2), n] = result.reshape(2, slots, features)
        for c in range(2):
            for k in range(1, tp_size):
                start(remote(
                    part_rows.at[first + c, peer(k)], landed.at[first + c, k],
                    p_send.at[d, c, k], p_recv.at[d, c, k], me, peer(k),
                ))

    def sum_rows(d):
        for c in range(2):
            source = behind(d, c)
            total = part_rows[source, part].astype(F32)
            for k in range(1, tp_size):
                here = landed.at[source, k]
                remote(here, here, p_send.at[d, c, k], p_recv.at[d, c, k], twin, part).wait_recv()
                total = total + landed[source, k].astype(F32)
            reduced[source] = total.astype(BF16)
            if d > 0:
                start(remote(
                    reduced.at[source], comb.at[me], r_send.at[d, c], r_recv.at[d, core], source, part
                ))
        if d == 0:
            comb[me] = reduced[me]
            start(remote(
                reduced.at[twin], comb.at[me], r_send.at[0, 0], r_recv.at[0, 0], twin, part
            ))

    order = [d for d in range(1, levels)]
    for d in order:
        pass_latents(d)
    for load in loads[3:6]:
        load.wait()
    run_expert(0)
    pending = list(order)
    if pending:
        pass_rows(pending.pop(0))
    for d in order:
        pass_latents_on(d)
    here = latent.at[twin]
    remote(here, here, ko_send.at[0], ko_recv.at[0], twin, part).wait_recv()
    for d in order:
        wait_latents(d)
    for load in loads[1:3]:
        load.wait()

    length = latent.shape[0] * latent.shape[1] * latent.shape[2]
    every = latent[...].reshape(length, latent.shape[3])
    keys = dot(every[:, :rank], v_key[...]).astype(BF16)
    vals[...] = dot(every[:, :rank], v_value[...]).astype(BF16)
    for h in range(heads):
        kcat[h, :, :NOPE] = keys[:, h * NOPE : (h + 1) * NOPE]
        kcat[h, :, NOPE:] = every[:, rank : rank + 128]
    factor = (NOPE + ROPE) ** (-0.5)
    for h in range(heads):
        if pending:
            pass_rows(pending.pop(0))
        score = lax.dot_general(
            qcat[h], kcat[h], (((1,), (1,)), ((), ())), preferred_element_type=F32
        ) * factor
        peak = jnp.max(score, -1, keepdims=True)
        weights = jnp.exp(score - peak)
        total = jnp.sum(weights, -1, keepdims=True)
        summed = dot(weights.astype(BF16), vals[:, h * VDIM : (h + 1) * VDIM])
        attended[:, h * VDIM : (h + 1) * VDIM] = (summed / total).astype(BF16)
    while pending:
        pass_rows(pending.pop(0))
    loads[6].wait()
    mix_part[...] = dot(attended[...], v_mix[...]).astype(BF16).reshape(mix_part.shape)
    for k in range(1, tp_size):
        start(remote(
            mix_part.at[peer(k)], mix_landed.at[k], m_send.at[k], m_recv.at[k], me, peer(k)
        ))

    for i, d in enumerate(order):
        run_expert(d)
        sum_rows(([0] + order)[i])

    total = mix_part[part].astype(F32)
    for k in range(1, tp_size):
        here = mix_landed.at[k]
        remote(here, here, m_send.at[k], m_recv.at[k], twin, part).wait_recv()
        total = total + mix_landed[k].astype(F32)
    mixed[...] = total.astype(BF16)

    sum_rows(([0] + order)[-1])
    here = comb.at[twin]
    remote(here, here, r_send.at[0, 0], r_recv.at[0, 0], twin, part).wait_recv()
    for d in order:
        for c in range(2):
            here = comb.at[lax.rem(level + d, levels) * 2 + c]
            remote(here, here, r_send.at[d, c], r_recv.at[d, c], twin, part).wait_recv()
    back = comb[...].reshape(ep_size * slots, features)
    seat = lax.broadcasted_iota(jnp.int32, (tokens, ep_size * slots), 1).astype(F32)
    result = jnp.zeros((tokens, features), F32)
    for k in range(choose):
        pick = jnp.where(seat == facts[:, k : k + 1], 1.0, 0.0).astype(BF16)
        result = result + dot(pick, back) * facts[:, choose + k : choose + k + 1]
    expert_out[...] = result.astype(BF16)
    for copy in waits:
        copy.wait_send()


def body(
    q_latent,
    kv_latent,
    rope_key,
    q_gain,
    kv_gain,
    w_query,
    w_key,
    w_value,
    w_mix_out,
    expert_in,
    norm_gain,
    routes,
    route_scores,
    w_gate,
    w_up,
    w_down,
):
    ep_size, tp_size = lax.axis_size("ep"), lax.axis_size("tp")
    levels = ep_size // 2
    tokens, width = expert_in.shape
    count = kv_latent.shape[0]
    choose = routes.shape[1]
    slots = 2 * choose * tokens // ep_size
    heads = w_query.shape[1] // (NOPE + ROPE)
    features = width // tp_size
    units = w_gate.shape[2]
    mine = count // tp_size
    padded = -(-mine // 16) * 16
    split = tp_size if padded == mine else 1
    queries = padded * tp_size

    positions = (lax.axis_index("ep") * count + jnp.arange(count, dtype=jnp.int32)).astype(F32)
    inverse = rope_base ** (-jnp.arange(0, ROPE, 2).astype(F32) / ROPE)
    phase = positions[:, None] * inverse[None, :]
    cosine, sine = jnp.cos(phase), jnp.sin(phase)
    table = jnp.concatenate([cosine] * 4 + [-sine, sine] * 2, 1)

    def pad_rows(values):
        if padded == mine:
            return values
        values = values.reshape(tp_size, mine, values.shape[1])
        return jnp.pad(values, ((0, 0), (0, padded - mine), (0, 0))).reshape(queries, -1)

    dma = pltpu.SemaphoreType.DMA
    vmem = pl.BlockSpec(memory_space=pltpu.VMEM)
    far = pl.BlockSpec(memory_space=pl.ANY)
    wide = latent_width = kv_latent.shape[1] + 128
    chunk = count // split
    mixed, expert_out = pl.pallas_call(
        functools.partial(layer_kernel, (ep_size, tp_size, slots, choose, heads, split)),
        out_shape=(
            jax.ShapeDtypeStruct((padded, width), BF16),
            jax.ShapeDtypeStruct((tokens, features), BF16),
        ),
        in_specs=[vmem] * 11 + [far] * 7,
        out_specs=(vmem, vmem),
        scratch_shapes=[
            pltpu.VMEM(w_query.shape, BF16),
            pltpu.VMEM(w_key.shape, BF16),
            pltpu.VMEM(w_value.shape, BF16),
            pltpu.VMEM(w_mix_out.shape, BF16),
            pltpu.VMEM((width, units), BF16),
            pltpu.VMEM((width, units), BF16),
            pltpu.VMEM((units, width), BF16),
            pltpu.VMEM((ep_size, split, chunk, latent_width), BF16),
            pltpu.VMEM((heads, ep_size * count, NOPE + 128), BF16),
            pltpu.VMEM((ep_size * count, heads * VDIM), BF16),
            pltpu.VMEM((heads, queries, NOPE + 128), BF16),
            pltpu.VMEM((queries, heads * VDIM), BF16),
            pltpu.VMEM((tp_size, padded, width), BF16),
            pltpu.VMEM((tp_size, padded, width), BF16),
            pltpu.VMEM((tokens, width), BF16),
            pltpu.VMEM((ep_size * slots, tokens), BF16),
            pltpu.VMEM((tokens, 128), F32),
            pltpu.VMEM((ep_size, slots, features), BF16),
            pltpu.VMEM((slots, width), BF16),
            pltpu.VMEM((ep_size, slots, width), BF16),
            pltpu.VMEM((2 * slots, units), BF16),
            pltpu.VMEM((ep_size, tp_size, slots, features), BF16),
            pltpu.VMEM((ep_size, tp_size, slots, features), BF16),
            pltpu.VMEM((ep_size, slots, features), BF16),
            pltpu.VMEM((ep_size, slots, features), BF16),
            dma((7,)),
            dma((levels,)), dma((levels,)),
            dma((levels, tp_size)), dma((levels, tp_size)),
            dma((levels, tp_size)), dma((levels, tp_size)),
            dma((1,)), dma((1,)),
            dma((levels, 2)), dma((levels, 2)),
            dma((levels, 2, tp_size)), dma((levels, 2, tp_size)),
            dma((1,)), dma((1,)),
            dma((levels, 2, tp_size)), dma((levels, 2, tp_size)),
            dma((levels, 2)), dma((levels, 2)),
            dma((tp_size,)), dma((tp_size,)),
        ],
        compiler_params=pltpu.CompilerParams(
            collective_id=0, has_side_effects=True, vmem_limit_bytes=60 * 1024 * 1024
        ),
    )(
        pad_rows(q_latent), kv_latent, rope_key, q_gain[None, :], kv_gain[None, :], table,
        pad_rows(table), expert_in, norm_gain[None, :], routes.T, route_scores.T,
        w_query, w_key, w_value, w_mix_out, w_gate[0], w_up[0], w_down[0],
    )
    return (mixed[:mine], expert_out)


def solution(mesh):
    in_specs = (
        P("ep", None),
        P("ep", None),
        P("ep", None),
        P(),
        P(),
        P(None, "tp"),
        P(None, "tp"),
        P(None, "tp"),
        P("tp", None),
        P("ep", None),
        P(),
        P("ep", None),
        P("ep", None),
        P("ep", None, "tp"),
        P("ep", None, "tp"),
        P("ep", "tp", None),
    )
    out_specs = (P(("ep", "tp"), None), P("ep", "tp"))
    return jax.shard_map(body, mesh=mesh, in_specs=in_specs, out_specs=out_specs, check_vma=False)
```

```python
import functools
import math

import jax
import jax.numpy as jnp
import numpy as np
from jax import lax
from jax.experimental import pallas as pl
from jax.experimental.pallas import tpu as pltpu
from jax.sharding import PartitionSpec as P

NOPE = 128
ROPE = 64
VDIM = 128

eps_norm = 1e-05
rope_base = 10000.0

MESH = pl.DeviceIdType.MESH
F32 = jnp.float32
BF16 = jnp.bfloat16


def remote(src, dst, send, recv, ep, tp):
    return pltpu.make_async_remote_copy(
        src_ref=src, dst_ref=dst, send_sem=send, recv_sem=recv, device_id=(ep, tp), device_id_type=MESH
    )


def dot(left, right):
    return jnp.dot(left, right, preferred_element_type=F32)


def rms_scale(values, gain):
    wide = values.astype(F32)
    return wide * lax.rsqrt(jnp.mean(wide * wide, -1, keepdims=True) + eps_norm) * gain


def rotate(values, angles, axis):
    source = lax.broadcasted_iota(jnp.int32, (ROPE, 256), 0)
    lane = lax.broadcasted_iota(jnp.int32, (ROPE, 256), 1)
    same = (lane < 128) & (source == lane % ROPE)
    turned = (lane >= 128) & (source == (lane + ROPE // 2) % ROPE)
    spread = jnp.where(same | turned, 1.0, 0.0).astype(BF16)
    wide = lax.dot_general(
        values, spread, (((axis,), (0,)), ((), ())), preferred_element_type=F32
    )
    return (wide[:, :128] * angles[0] + wide[:, 128:] * angles[1]).astype(BF16)


def layer_kernel(
    sizes,
    q_lat, kv_lat, rope_key, q_gain, kv_gain, near_angle, far_angle, expert_in, norm_gain, routes, scores,
    w_query, w_key, w_value, w_mix, w_gate, w_up, w_down,
    mixed_far, expert_far,
    mixed, expert_out, v_query, v_key, v_value, v_mix, v_gate, v_up, v_down,
    latent, turned, kcat, vals, qcat, attended, mix_part, mix_first, mix_pair, mix_second,
    normed, place, facts, send_rows, twin_rows, rows, hidden, part_rows, first_rows, pair_rows, second_rows,
    reduced, comb,
    w_sem, kz_send, kz_recv, kc_send, kc_recv, ko_send, ko_recv,
    dz_send, dz_recv, dt_send, dt_recv, do_send, do_recv,
    p_send, p_recv, q_send, q_recv, r_send, r_recv, m_send, m_recv, n_send, n_recv,
):
    ep_size, tp_size, slots, choose, heads, extent = sizes
    levels = ep_size // 2
    me = lax.axis_index("ep")
    part = lax.axis_index("tp")
    level, core = me // 2, me % 2
    twin = level * 2 + 1 - core
    spot_of = (part % extent[0], part // extent[0])
    tokens, width = expert_in.shape
    features = width // tp_size
    rank = kv_lat.shape[1]
    waits = []

    def start(copy):
        copy.start()
        waits.append(copy)

    def columns(index):
        return pl.ds(pl.multiple_of(index * features, features), features)

    def step(axis, k):
        return lax.rem(spot_of[axis] + k, extent[axis])

    def at(axis, first, second):
        return second * extent[0] + first if axis == 0 else first * extent[0] + second

    def facing(d):
        if levels & (levels - 1):
            return lax.rem(level + d, levels), lax.rem(level - d + levels, levels)
        other = level
        bit = 1
        while bit < levels:
            if d & bit:
                other = other + bit * (1 - 2 * (level // bit % 2))
            bit *= 2
        return other, other

    barrier = pltpu.get_barrier_semaphore()
    for d in range(1, ep_size):
        pl.semaphore_signal(
            barrier, inc=1, device_id=(lax.rem(me + d, ep_size), part), device_id_type=MESH
        )
    for k in range(1, tp_size):
        pl.semaphore_signal(
            barrier, inc=1, device_id=(me, lax.rem(part + k, tp_size)), device_id_type=MESH
        )
    loads = [
        pltpu.make_async_copy(src, dst, w_sem.at[i])
        for i, (src, dst) in enumerate((
            (w_query, v_query), (w_gate, v_gate), (w_up, v_up), (w_down, v_down),
            (w_key, v_key), (w_value, v_value), (w_mix, v_mix),
        ))
    ]
    loads[0].start()

    count = kv_lat.shape[0]
    block_cosine = far_angle[me][:, :128]
    block_sine = far_angle[me][:, 128:]

    def turn_by(first, last):
        own_cosine, own_sine = near_angle[first:last, :128], near_angle[first:last, 128:]
        lane = lax.broadcasted_iota(jnp.int32, own_sine.shape, 1)
        sine = block_sine * own_cosine + block_cosine * own_sine
        return (
            block_cosine * own_cosine - block_sine * own_sine,
            jnp.where(lane % ROPE < ROPE // 2, -sine, sine),
        )

    angles = turn_by(0, count)
    angles_q = angles if q_lat.shape[0] == count else turn_by(count, count + q_lat.shape[0])
    kv_normed = rms_scale(kv_lat[...], kv_gain[...]).astype(BF16)
    key_turned = rotate(rope_key[...], angles, 0)
    latent[me] = kv_normed
    low = lax.broadcasted_iota(jnp.int32, (count // 2, 128), 1) < ROPE
    turned[me] = jnp.where(low, key_turned[: count // 2], key_turned[count // 2 :])

    for load in loads[1:]:
        load.start()
    named = routes[...]
    experts = max(8, ep_size)
    expert = lax.broadcasted_iota(jnp.int32, (experts, tokens), 0)
    member = [expert == named[k : k + 1, :] for k in range(choose)]
    any_member = member[0]
    for k in range(1, choose):
        any_member = any_member | member[k]
    earlier = lax.broadcasted_iota(jnp.int32, (tokens, tokens), 0) < lax.broadcasted_iota(
        jnp.int32, (tokens, tokens), 1
    )
    before = dot(
        jnp.where(any_member, 1.0, 0.0).astype(BF16), jnp.where(earlier, 1.0, 0.0).astype(BF16)
    )
    spot = before + (expert * slots).astype(F32)
    targets = [
        jnp.sum(jnp.where(member[k], spot, 0.0), 0, keepdims=True) for k in range(choose)
    ]
    score = scores[...]
    shares = score / jnp.sum(score, 0, keepdims=True)
    known = jnp.concatenate(targets + [shares], 0)
    known = jnp.concatenate([known, jnp.zeros((128 - 2 * choose, tokens), F32)], 0)
    facts[...] = jnp.transpose(known)
    seat = lax.broadcasted_iota(jnp.int32, (ep_size * slots, tokens), 0).astype(F32)
    chosen = seat == targets[0]
    for k in range(1, choose):
        chosen = chosen | (seat == targets[k])
    place[...] = jnp.where(chosen, 1.0, 0.0).astype(BF16)

    wide = expert_in[...].astype(F32)
    centered = wide - jnp.mean(wide, -1, keepdims=True)
    normed[...] = (
        centered
        * lax.rsqrt(jnp.mean(centered * centered, -1, keepdims=True) + eps_norm)
        * norm_gain[...]
    ).astype(BF16)


    def seats(index):
        return place[pl.ds(pl.multiple_of(index * slots, slots), slots), :]

    send_rows[...] = dot(place[...], normed[:, columns(part)]).astype(BF16).reshape(send_rows.shape)
    twin_rows[...] = dot(seats(twin), normed[...]).astype(BF16)
    rows[me] = dot(seats(me), normed[...]).astype(BF16)

    pl.semaphore_wait(barrier, ep_size + tp_size - 2)

    outs = [
        pltpu.make_async_copy(mixed, mixed_far, w_sem.at[7]),
        pltpu.make_async_copy(expert_out, expert_far, w_sem.at[8]),
    ]
    near = list(range(1, levels))
    order = near[:1] + near[:0:-1]
    start(remote(twin_rows, rows.at[me], do_send.at[0], do_recv.at[0], twin, part))
    for i, whole in enumerate((latent, turned)):
        start(remote(whole.at[me], whole.at[me], ko_send.at[i], ko_recv.at[i], twin, part))

    class Share:
        def __init__(self, view, sends, recvs, axis):
            self.view, self.sends, self.recvs, self.axis = view, sends, recvs, axis
            self.first, self.second = extent[axis], extent[1 - axis]

        def number(self, k, j):
            if j == 0:
                return k - 1
            if k == 0:
                return self.first - 1 + j - 1
            return self.first + self.second - 2 + (k - 1) * (self.second - 1) + j - 1

        def index(self, k, j):
            axis = self.axis
            return at(axis, step(axis, self.first - k if k else 0), step(1 - axis, self.second - j if j else 0))

        def push(self, here, k, j, target):
            number = self.number(k, j)
            start(remote(here, here, self.sends(number), self.recvs(number), me, target))

        def arrive(self, k, j):
            number, index = self.number(k, j), self.index(k, j)
            here = self.view(index)
            remote(here, here, self.sends(number), self.recvs(number), twin, part).wait_recv()
            return here

        def direct(self):
            axis, here = self.axis, self.view(part)
            for k in range(1, self.first):
                self.push(here, k, 0, at(axis, step(axis, k), spot_of[1 - axis]))
            for j in range(1, self.second):
                self.push(here, 0, j, at(axis, spot_of[axis], step(1 - axis, j)))

        def relay(self):
            axis = self.axis
            for k in range(1, self.first):
                here = self.arrive(k, 0)
                for j in range(1, self.second):
                    self.push(here, k, j, at(axis, spot_of[axis], step(1 - axis, j)))

        def finish(self):
            for j in range(1, self.second):
                for k in range(self.first):
                    self.arrive(k, j)

    class Sum:
        def __init__(self, whole, one, pair, two, s1, r1, s2, r2, axis):
            self.whole, self.one, self.pair, self.two = whole, one, pair, two
            self.s1, self.r1, self.s2, self.r2, self.axis = s1, r1, s2, r2, axis
            self.first, self.second = extent[axis], extent[1 - axis]

        def strip(self, index):
            return self.whole.at[:, index] if self.axis == 0 else self.whole.at[index]

        def begin(self):
            axis = self.axis
            for k in range(1, self.first):
                start(remote(
                    self.strip(step(axis, k)), self.one.at[k - 1, pl.ds(0, self.second)],
                    self.s1(k - 1), self.r1(k - 1),
                    me, at(axis, step(axis, k), spot_of[1 - axis]),
                ))

        def part_sum(self, j):
            axis = self.axis
            row = step(1 - axis, j)
            mine = self.whole[row, spot_of[0]] if axis == 0 else self.whole[spot_of[1], row]
            total = mine.astype(F32)
            for k in range(1, self.first):
                total = total + self.one[k - 1, row].astype(F32)
            return total

        def middle(self):
            axis = self.axis
            for k in range(1, self.first):
                here = self.one.at[k - 1, pl.ds(0, self.second)]
                remote(here, here, self.s1(k - 1), self.r1(k - 1), twin, part).wait_recv()
            for j in range(1, self.second):
                self.pair[j - 1] = self.part_sum(j).astype(BF16)
            for j in range(1, self.second):
                start(remote(
                    self.pair.at[j - 1], self.two.at[j - 1], self.s2(j - 1), self.r2(j - 1),
                    me, at(axis, spot_of[axis], step(1 - axis, j)),
                ))

        def end(self):
            total = self.part_sum(0)
            for j in range(1, self.second):
                here = self.two.at[j - 1]
                remote(here, here, self.s2(j - 1), self.r2(j - 1), twin, part).wait_recv()
                total = total + self.two[j - 1].astype(F32)
            return total

    def latent_send(d):
        target = facing(d)[0] * 2 + core
        for i, whole in enumerate((latent, turned)):
            here = whole.at[me]
            start(remote(here, here, kz_send.at[d, i], kz_recv.at[d, i], target, part))

    def latent_pass(d):
        for i, whole in enumerate((latent, turned)):
            here = whole.at[facing(d)[1] * 2 + core]
            remote(here, here, kz_send.at[d, i], kz_recv.at[d, i], twin, part).wait_recv()
            start(remote(here, here, kc_send.at[d, i], kc_recv.at[d, i], twin, part))

    def latent_twin(d):
        for i, whole in enumerate((latent, turned)):
            if d == 0:
                here = whole.at[twin]
                remote(here, here, ko_send.at[i], ko_recv.at[i], twin, part).wait_recv()
            else:
                here = whole.at[facing(d)[1] * 2 + 1 - core]
                remote(here, here, kc_send.at[d, i], kc_recv.at[d, i], twin, part).wait_recv()

    def row_send(d, cores=(0, 1)):
        for c in cores:
            target = facing(d)[0] * 2 + c
            start(remote(
                send_rows.at[target], rows.at[me, :, columns(part)],
                dz_send.at[d, c], dz_recv.at[d, core], target, part,
            ))

    def row_share(d, c):
        block = facing(d)[1] * 2 + c
        return Share(
            lambda index: rows.at[block, :, columns(index)],
            lambda n: dt_send.at[d, c, n], lambda n: dt_recv.at[d, c, n], c,
        )

    def row_direct(d, cores=(0, 1)):
        for c in cores:
            here = rows.at[facing(d)[1] * 2 + c, :, columns(part)]
            remote(here, here, dz_send.at[d, c], dz_recv.at[d, c], twin, part).wait_recv()
            row_share(d, c).direct()

    def row_relay(d):
        for c in range(2):
            row_share(d, c).relay()

    def row_finish(d):
        if d == 0:
            here = rows.at[twin]
            remote(here, here, do_send.at[0], do_recv.at[0], twin, part).wait_recv()
            return
        for c in range(2):
            row_share(d, c).finish()

    def row_sum(d, c):
        block = facing(d)[1] * 2 + c
        return Sum(
            part_rows.at[block], first_rows.at[block], pair_rows.at[block], second_rows.at[block],
            lambda n: p_send.at[d, c, n], lambda n: p_recv.at[d, c, n],
            lambda n: q_send.at[d, c, n], lambda n: q_recv.at[d, c, n], c,
        )

    block = min(256, v_gate.shape[1])

    def run_expert(d):
        first = facing(d)[1] * 2
        arrived = rows[pl.ds(first, 2)].reshape(2 * slots, width)
        for j in range(v_gate.shape[1] // block):
            units = slice(j * block, (j + 1) * block)
            gate = dot(arrived, v_gate[:, units])
            up = dot(arrived, v_up[:, units])
            hidden[:, units] = (gate / (1.0 + jnp.exp(-gate)) * up).astype(BF16)
        for n in range(tp_size):
            result = dot(hidden[...], v_down[:, n * features : (n + 1) * features]).astype(BF16)
            part_rows[pl.ds(first, 2), n // extent[0], n % extent[0]] = result.reshape(2, slots, features)

    def sum_begin(d):
        for c in range(2):
            row_sum(d, c).begin()

    def sum_middle(d):
        for c in range(2):
            row_sum(d, c).middle()

    def sum_end(d):
        other = facing(d)[1]
        for c in range(2):
            reduced[other * 2 + c] = row_sum(d, c).end().astype(BF16)
        if d == 0:
            comb[me] = reduced[me]
            start(remote(reduced.at[twin], comb.at[me], r_send.at[0, 0], r_recv.at[0, 0], twin, part))
            return
        for c in range(2):
            source = other * 2 + c
            start(remote(
                reduced.at[source], comb.at[me], r_send.at[d, c], r_recv.at[d, core], source, part
            ))

    def mix_sum(h):
        return Sum(
            mix_part.at[h], mix_first.at[h], mix_pair.at[h], mix_second.at[h],
            lambda n: m_send.at[h, n], lambda n: m_recv.at[h, n],
            lambda n: n_send.at[h, n], lambda n: n_recv.at[h, n], h,
        )

    def queries():
        loads[0].wait()
        q_normed = rms_scale(q_lat[...], q_gain[...]).astype(BF16)
        query = dot(q_normed, v_query[...])
        for h in range(heads):
            base = h * (NOPE + ROPE)
            qcat[h, :, :NOPE] = query[:, base : base + NOPE].astype(BF16)
            turn = query[:, base + NOPE : base + NOPE + ROPE].astype(BF16)
            qcat[h, :, NOPE:] = rotate(turn, angles_q, 1)

    def make_keys(d):
        first = facing(d)[1] * 2
        span = 2 * count
        tokens_in = pl.ds(pl.multiple_of(first * count, span), span)
        some = latent[pl.ds(first, 2)].reshape(span, rank)
        keys = dot(some, v_key[...]).astype(BF16)
        vals[tokens_in, :] = dot(some, v_value[...]).astype(BF16)
        both = turned[pl.ds(first, 2)]
        low = lax.broadcasted_iota(jnp.int32, both.shape, 2) < ROPE
        none = jnp.zeros_like(both)
        spread = jnp.concatenate([jnp.where(low, both, none), jnp.where(low, none, both)], 1)
        for h in range(heads):
            kcat[h, tokens_in, :NOPE] = keys[:, h * NOPE : (h + 1) * NOPE]
            kcat[h, tokens_in, NOPE:] = spread.reshape(span, 128)

    def attend(h):
        factor = (NOPE + ROPE) ** (-0.5)
        score = lax.dot_general(
            qcat[h], kcat[h], (((1,), (1,)), ((), ())), preferred_element_type=F32
        ) * factor
        peak = jnp.max(score, -1, keepdims=True)
        weights = jnp.exp(score - peak)
        total = jnp.sum(weights, -1, keepdims=True)
        summed = dot(weights.astype(BF16), vals[:, h * VDIM : (h + 1) * VDIM])
        attended[:, h * VDIM : (h + 1) * VDIM] = (summed / total).astype(BF16)

    def make_mix():
        loads[6].wait()
        half = width // 2
        for h in range(2):
            result = dot(attended[...], v_mix[:, h * half : (h + 1) * half]).astype(BF16)
            mix_part[h] = result.reshape(mix_part.shape[1:])
        for h in range(2):
            mix_sum(h).begin()

    def mix_middle():
        for h in range(2):
            mix_sum(h).middle()

    def mix_end():
        half = width // 2
        for h in range(2):
            mixed[:, h * half : (h + 1) * half] = mix_sum(h).end().astype(BF16)
        outs[0].start()

    rest = order[1:]
    for d in order[:1]:
        row_send(d)
    queries()
    for d in rest[:1]:
        row_send(d)
    for load in loads[4:6]:
        load.wait()
    latent_twin(0)
    make_keys(0)
    for load in loads[1:4]:
        load.wait()
    row_finish(0)
    run_expert(0)
    for d in order[:1]:
        row_direct(d)
    sum_begin(0)
    for d in rest[1:]:
        row_send(d)
    for d in near:
        latent_send(d)
    for d in rest[:1]:
        row_direct(d)
    for d in order[:1]:
        row_relay(d)
    sum_middle(0)
    groups = [0] + order
    last = len(order) - 1
    for i, d in enumerate(order):
        if i == last:
            for e in near:
                latent_pass(e)
            for e in near:
                latent_twin(e)
                make_keys(e)
        row_finish(d)
        if i + 1 < last:
            row_relay(order[i + 1])
        if i + 2 <= last:
            row_direct(order[i + 2])
        run_expert(d)
        sum_begin(d)
        if i + 1 == last:
            row_relay(order[last])
        if i > 0:
            sum_middle(groups[i])
            sum_end(groups[i - 1])
    for h in range(heads):
        attend(h)
    make_mix()
    for d in order[-1:]:
        sum_middle(d)
    for d in groups[max(0, len(groups) - 2) : -1]:
        sum_end(d)
    sum_end(groups[-1])
    mix_middle()
    mix_end()

    here = comb.at[twin]
    remote(here, here, r_send.at[0, 0], r_recv.at[0, 0], twin, part).wait_recv()
    for d in order:
        for c in range(2):
            here = comb.at[facing(d)[0] * 2 + c]
            remote(here, here, r_send.at[d, c], r_recv.at[d, c], twin, part).wait_recv()
    back = comb[...].reshape(ep_size * slots, features)
    seat = lax.broadcasted_iota(jnp.int32, (tokens, ep_size * slots), 1).astype(F32)
    result = jnp.zeros((tokens, features), F32)
    for k in range(choose):
        pick = jnp.where(seat == facts[:, k : k + 1], 1.0, 0.0).astype(BF16)
        result = result + dot(pick, back) * facts[:, choose + k : choose + k + 1]
    expert_out[...] = result.astype(BF16)
    outs[1].start()
    for copy in waits:
        copy.wait_send()
    for out in outs:
        out.wait()


def hand_over(mixed_in, expert_in, mixed, expert_out):
    mixed[...] = mixed_in[: mixed.shape[0]]
    expert_out[...] = expert_in[...]


def body(
    q_latent,
    kv_latent,
    rope_key,
    q_gain,
    kv_gain,
    w_query,
    w_key,
    w_value,
    w_mix_out,
    expert_in,
    norm_gain,
    routes,
    route_scores,
    w_gate,
    w_up,
    w_down,
):
    ep_size, tp_size = lax.axis_size("ep"), lax.axis_size("tp")
    levels = ep_size // 2
    tokens, width = expert_in.shape
    count = kv_latent.shape[0]
    choose = routes.shape[1]
    slots = 2 * choose * tokens // ep_size
    heads = w_query.shape[1] // (NOPE + ROPE)
    features = width // tp_size
    units = w_gate.shape[2]
    mine = count // tp_size
    padded = -(-mine // 16) * 16
    queries = padded * tp_size
    narrow = math.isqrt(tp_size)
    while tp_size % narrow:
        narrow -= 1
    extent = (tp_size // narrow, narrow)
    most = max(extent)
    ahead = max(1, most - 1)
    wing = width // 2

    lane = np.arange(128) % (ROPE // 2)
    inverse = np.float32(rope_base) ** (-(2 * lane).astype(np.float32) / np.float32(ROPE))

    def turns(positions):
        phase = positions[:, None].astype(np.float64) * inverse[None, :].astype(np.float64)
        return np.concatenate([np.cos(phase), np.sin(phase)], 1).astype(np.float32)

    near_angle = turns(np.arange(count))
    if padded != mine:
        spread = np.pad(near_angle.reshape(tp_size, mine, 256), ((0, 0), (0, padded - mine), (0, 0)))
        near_angle = np.concatenate([near_angle, spread.reshape(queries, 256)], 0)
    far_angle = turns(np.arange(ep_size) * count)[:, None, :]

    def pad_rows(values):
        if padded == mine:
            return values
        values = values.reshape(tp_size, mine, values.shape[1])
        return jnp.pad(values, ((0, 0), (0, padded - mine), (0, 0))).reshape(queries, -1)

    dma = pltpu.SemaphoreType.DMA
    vmem = pl.BlockSpec(memory_space=pltpu.VMEM)
    far = pl.BlockSpec(memory_space=pl.ANY)
    mixed, expert_out = pl.pallas_call(
        functools.partial(layer_kernel, (ep_size, tp_size, slots, choose, heads, extent)),
        out_shape=(
            jax.ShapeDtypeStruct((padded, width), BF16),
            jax.ShapeDtypeStruct((tokens, features), BF16),
        ),
        in_specs=[vmem] * 11 + [far] * 7,
        out_specs=(far, far),
        scratch_shapes=[
            pltpu.VMEM((padded, width), BF16),
            pltpu.VMEM((tokens, features), BF16),
            pltpu.VMEM(w_query.shape, BF16),
            pltpu.VMEM(w_key.shape, BF16),
            pltpu.VMEM(w_value.shape, BF16),
            pltpu.VMEM(w_mix_out.shape, BF16),
            pltpu.VMEM((width, units), BF16),
            pltpu.VMEM((width, units), BF16),
            pltpu.VMEM((units, width), BF16),
            pltpu.VMEM((ep_size, count, kv_latent.shape[1]), BF16),
            pltpu.VMEM((ep_size, count // 2, 128), BF16),
            pltpu.VMEM((heads, ep_size * count, NOPE + 128), BF16),
            pltpu.VMEM((ep_size * count, heads * VDIM), BF16),
            pltpu.VMEM((heads, queries, NOPE + 128), BF16),
            pltpu.VMEM((queries, heads * VDIM), BF16),
            pltpu.VMEM((2, extent[1], extent[0], padded, wing), BF16),
            pltpu.VMEM((2, ahead, most, padded, wing), BF16),
            pltpu.VMEM((2, ahead, padded, wing), BF16),
            pltpu.VMEM((2, ahead, padded, wing), BF16),
            pltpu.VMEM((tokens, width), BF16),
            pltpu.VMEM((ep_size * slots, tokens), BF16),
            pltpu.VMEM((tokens, 128), F32),
            pltpu.VMEM((ep_size, slots, features), BF16),
            pltpu.VMEM((slots, width), BF16),
            pltpu.VMEM((ep_size, slots, width), BF16),
            pltpu.VMEM((2 * slots, units), BF16),
            pltpu.VMEM((ep_size, extent[1], extent[0], slots, features), BF16),
            pltpu.VMEM((ep_size, ahead, most, slots, features), BF16),
            pltpu.VMEM((ep_size, ahead, slots, features), BF16),
            pltpu.VMEM((ep_size, ahead, slots, features), BF16),
            pltpu.VMEM((ep_size, slots, features), BF16),
            pltpu.VMEM((ep_size, slots, features), BF16),
            dma((9,)),
            dma((levels, 2)), dma((levels, 2)),
            dma((levels, 2)), dma((levels, 2)),
            dma((2,)), dma((2,)),
            dma((levels, 2)), dma((levels, 2)),
            dma((levels, 2, tp_size)), dma((levels, 2, tp_size)),
            dma((1,)), dma((1,)),
            dma((levels, 2, ahead)), dma((levels, 2, ahead)),
            dma((levels, 2, ahead)), dma((levels, 2, ahead)),
            dma((levels, 2)), dma((levels, 2)),
            dma((2, ahead)), dma((2, ahead)),
            dma((2, ahead)), dma((2, ahead)),
        ],
        compiler_params=pltpu.CompilerParams(
            collective_id=0, has_side_effects=True, vmem_limit_bytes=60 * 1024 * 1024
        ),
    )(
        pad_rows(q_latent), kv_latent, rope_key.T, q_gain[None, :], kv_gain[None, :], near_angle, far_angle,
        expert_in, norm_gain[None, :], routes.T, route_scores.T,
        w_query, w_key, w_value, w_mix_out, w_gate[0], w_up[0], w_down[0],
    )
    return pl.pallas_call(
        hand_over,
        out_shape=(
            jax.ShapeDtypeStruct((mine, width), BF16),
            jax.ShapeDtypeStruct((tokens, features), BF16),
        ),
        in_specs=[vmem] * 2,
        out_specs=(vmem, vmem),
    )(mixed, expert_out)


def solution(mesh):
    in_specs = (
        P("ep", None),
        P("ep", None),
        P("ep", None),
        P(),
        P(),
        P(None, "tp"),
        P(None, "tp"),
        P(None, "tp"),
        P("tp", None),
        P("ep", None),
        P(),
        P("ep", None),
        P("ep", None),
        P("ep", None, "tp"),
        P("ep", None, "tp"),
        P("ep", "tp", None),
    )
    out_specs = (P(("ep", "tp"), None), P("ep", "tp"))
    return jax.shard_map(body, mesh=mesh, in_specs=in_specs, out_specs=out_specs, check_vma=False)
```

```python
import functools
import math

import jax
import jax.numpy as jnp
import numpy as np
from jax import lax
from jax.experimental import pallas as pl
from jax.experimental.pallas import tpu as pltpu
from jax.sharding import PartitionSpec as P

NOPE = 128
ROPE = 64
VDIM = 128

eps_norm = 1e-05
rope_base = 10000.0

MESH = pl.DeviceIdType.MESH
F32 = jnp.float32
BF16 = jnp.bfloat16


def remote(src, dst, send, recv, ep, tp):
    return pltpu.make_async_remote_copy(
        src_ref=src, dst_ref=dst, send_sem=send, recv_sem=recv, device_id=(ep, tp), device_id_type=MESH
    )


def dot(left, right):
    return jnp.dot(left, right, preferred_element_type=F32)


def rms_scale(values, gain):
    wide = values.astype(F32)
    return wide * lax.rsqrt(jnp.mean(wide * wide, -1, keepdims=True) + eps_norm) * gain


def rotate(values, angles, axis):
    source = lax.broadcasted_iota(jnp.int32, (ROPE, 256), 0)
    lane = lax.broadcasted_iota(jnp.int32, (ROPE, 256), 1)
    same = (lane < 128) & (source == lane % ROPE)
    turned = (lane >= 128) & (source == (lane + ROPE // 2) % ROPE)
    spread = jnp.where(same | turned, 1.0, 0.0).astype(BF16)
    wide = lax.dot_general(
        values, spread, (((axis,), (0,)), ((), ())), preferred_element_type=F32
    )
    return (wide[:, :128] * angles[0] + wide[:, 128:] * angles[1]).astype(BF16)


def layer_kernel(
    sizes,
    h_q_lat, h_kv_lat, h_rope_key, h_q_gain, h_kv_gain, h_near_angle, h_far_angle, h_expert_in, h_norm_gain, h_routes, h_scores,
    w_query, w_key, w_value, w_mix, w_gate, w_up, w_down,
    mixed_far, expert_far,
    mixed, expert_out, q_lat, kv_lat, rope_key, q_gain, kv_gain, near_angle, far_angle, expert_in, norm_gain, routes, scores,
    v_query, v_key, v_value, v_mix, v_gate, v_up, v_down,
    latent, turned, kcat, vals, qcat, attended, mix_part, mix_first, mix_pair, mix_second,
    normed, place, facts, send_rows, twin_rows, rows, hidden, part_rows, first_rows, pair_rows, second_rows,
    reduced, comb,
    w_sem, i_sem, pool, kz_recv, kx_recv, kc_recv, ko_recv, dz_recv, dt_recv, do_recv, p_recv, q_recv, r_recv, m_recv, n_recv,
):
    ep_size, tp_size, slots, choose, heads, extent = sizes
    levels = ep_size // 2
    me = lax.axis_index("ep")
    part = lax.axis_index("tp")
    level, core = me // 2, me % 2
    twin = level * 2 + 1 - core
    spot_of = (part % extent[0], part // extent[0])
    tokens, width = expert_in.shape
    features = width // tp_size
    count, rank = kv_lat.shape
    waits = []
    spun = [None]

    def start(src, dst, recv, ep, tp):
        slot = len(waits) % pool.shape[0]
        if len(waits) >= pool.shape[0]:
            waits[len(waits) - pool.shape[0]].wait_send()
        copy = remote(src, dst, pool.at[slot], recv, ep, tp)
        copy.start()
        waits.append(copy)

    def landed(here, recv):
        remote(here, here, pool.at[0], recv, twin, part).wait_recv()

    def columns(index):
        return pl.ds(pl.multiple_of(index * features, features), features)

    def step(axis, k):
        return lax.rem(spot_of[axis] + k, extent[axis])

    def at(axis, first, second):
        return second * extent[0] + first if axis == 0 else first * extent[0] + second

    def facing(d):
        if levels & (levels - 1):
            return lax.rem(level + d, levels), lax.rem(level - d + levels, levels)
        other = level
        bit = 1
        while bit < levels:
            if d & bit:
                other = other + bit * (1 - 2 * (level // bit % 2))
            bit *= 2
        return other, other

    small = [
        pltpu.make_async_copy(src, dst, i_sem.at[i])
        for i, (src, dst) in enumerate((
            (h_kv_lat, kv_lat), (h_rope_key, rope_key), (h_kv_gain, kv_gain), (h_near_angle, near_angle),
            (h_far_angle, far_angle), (h_routes, routes), (h_scores, scores), (h_expert_in, expert_in),
            (h_norm_gain, norm_gain), (h_q_lat, q_lat), (h_q_gain, q_gain),
        ))
    ]
    for load in small[5:9] + small[:5] + small[9:]:
        load.start()
    barrier = pltpu.get_barrier_semaphore()
    for d in range(1, ep_size):
        pl.semaphore_signal(
            barrier, inc=1, device_id=(lax.rem(me + d, ep_size), part), device_id_type=MESH
        )
    for k in range(1, tp_size):
        pl.semaphore_signal(
            barrier, inc=1, device_id=(me, lax.rem(part + k, tp_size)), device_id_type=MESH
        )
    loads = [
        pltpu.make_async_copy(src, dst, w_sem.at[i])
        for i, (src, dst) in enumerate((
            (w_query, v_query), (w_gate, v_gate), (w_up, v_up), (w_down, v_down),
            (w_key, v_key), (w_value, v_value), (w_mix, v_mix),
        ))
    ]
    for i in (4, 5, 0, 1):
        loads[i].start()

    for load in small[5:9]:
        load.wait()
    for i in (2, 3, 6):
        loads[i].start()

    named = routes[...]
    experts = max(8, ep_size)
    expert = lax.broadcasted_iota(jnp.int32, (experts, tokens), 0)
    member = [expert == named[k : k + 1, :] for k in range(choose)]
    any_member = member[0]
    for k in range(1, choose):
        any_member = any_member | member[k]
    earlier = lax.broadcasted_iota(jnp.int32, (tokens, tokens), 0) < lax.broadcasted_iota(
        jnp.int32, (tokens, tokens), 1
    )
    before = dot(
        jnp.where(any_member, 1.0, 0.0).astype(BF16), jnp.where(earlier, 1.0, 0.0).astype(BF16)
    )
    spot = before + (expert * slots).astype(F32)
    targets = [
        jnp.sum(jnp.where(member[k], spot, 0.0), 0, keepdims=True) for k in range(choose)
    ]
    score = scores[...]
    shares = score / jnp.sum(score, 0, keepdims=True)
    known = jnp.concatenate(targets + [shares], 0)
    known = jnp.concatenate([known, jnp.zeros((128 - 2 * choose, tokens), F32)], 0)
    facts[...] = jnp.transpose(known)
    seat = lax.broadcasted_iota(jnp.int32, (ep_size * slots, tokens), 0).astype(F32)
    chosen = seat == targets[0]
    for k in range(1, choose):
        chosen = chosen | (seat == targets[k])
    place[...] = jnp.where(chosen, 1.0, 0.0).astype(BF16)

    wide = expert_in[...].astype(F32)
    centered = wide - jnp.mean(wide, -1, keepdims=True)
    normed[...] = (
        centered
        * lax.rsqrt(jnp.mean(centered * centered, -1, keepdims=True) + eps_norm)
        * norm_gain[...]
    ).astype(BF16)


    def seats(index):
        return place[pl.ds(pl.multiple_of(index * slots, slots), slots), :]

    send_rows[...] = dot(place[...], normed[:, columns(part)]).astype(BF16).reshape(send_rows.shape)
    twin_rows[...] = dot(seats(twin), normed[...]).astype(BF16)
    rows[me] = dot(seats(me), normed[...]).astype(BF16)

    pl.semaphore_wait(barrier, ep_size + tp_size - 2)

    outs = [
        pltpu.make_async_copy(mixed, mixed_far, w_sem.at[0]),
        pltpu.make_async_copy(expert_out, expert_far, w_sem.at[1]),
    ]
    near = list(range(1, levels))
    order = near[::-1]
    start(twin_rows, rows.at[me], do_recv.at[0], twin, part)

    def prepare_latents():
        for load in small[:5]:
            load.wait()
        block_cosine = far_angle[me][:, :128]
        block_sine = far_angle[me][:, 128:]

        def turn_by(first, last):
            own_cosine, own_sine = near_angle[first:last, :128], near_angle[first:last, 128:]
            lane = lax.broadcasted_iota(jnp.int32, own_sine.shape, 1)
            sine = block_sine * own_cosine + block_cosine * own_sine
            return (
                block_cosine * own_cosine - block_sine * own_sine,
                jnp.where(lane % ROPE < ROPE // 2, -sine, sine),
            )

        angles = turn_by(0, count)
        spun[0] = angles if q_lat.shape[0] == count else turn_by(count, count + q_lat.shape[0])
        kv_normed = rms_scale(kv_lat[...], kv_gain[...]).astype(BF16)
        key_turned = rotate(rope_key[...], angles, 0)
        latent[me] = kv_normed.reshape(latent.shape[1:])
        low = lax.broadcasted_iota(jnp.int32, (count // 2, 128), 1) < ROPE
        turned[me] = jnp.where(low, key_turned[: count // 2], key_turned[count // 2 :])
        for i, whole in enumerate((latent, turned)):
            start(whole.at[me], whole.at[me], ko_recv.at[i], twin, part)

    class Share:
        def __init__(self, view, recvs, axis):
            self.view, self.recvs, self.axis = view, recvs, axis
            self.first, self.second = extent[axis], extent[1 - axis]

        def number(self, k, j):
            if j == 0:
                return k - 1
            if k == 0:
                return self.first - 1 + j - 1
            return self.first + self.second - 2 + (k - 1) * (self.second - 1) + j - 1

        def index(self, k, j):
            axis = self.axis
            return at(axis, step(axis, self.first - k if k else 0), step(1 - axis, self.second - j if j else 0))

        def push(self, here, k, j, target):
            number = self.number(k, j)
            start(here, here, self.recvs(number), me, target)

        def arrive(self, k, j):
            number, index = self.number(k, j), self.index(k, j)
            here = self.view(index)
            landed(here, self.recvs(number))
            return here

        def direct(self):
            axis, here = self.axis, self.view(part)
            for k in range(1, self.first):
                self.push(here, k, 0, at(axis, step(axis, k), spot_of[1 - axis]))
            for j in range(1, self.second):
                self.push(here, 0, j, at(axis, spot_of[axis], step(1 - axis, j)))

        def relay(self):
            axis = self.axis
            for k in range(1, self.first):
                here = self.arrive(k, 0)
                for j in range(1, self.second):
                    self.push(here, k, j, at(axis, spot_of[axis], step(1 - axis, j)))

        def finish(self):
            for j in range(1, self.second):
                for k in range(self.first):
                    self.arrive(k, j)

    class Sum:
        def __init__(self, whole, one, pair, two, r1, r2, axis):
            self.whole, self.one, self.pair, self.two = whole, one, pair, two
            self.r1, self.r2, self.axis = r1, r2, axis
            self.first, self.second = extent[axis], extent[1 - axis]

        def strip(self, index):
            return self.whole.at[:, index] if self.axis == 0 else self.whole.at[index]

        def begin(self):
            axis = self.axis
            for k in range(1, self.first):
                start(
                    self.strip(step(axis, k)), self.one.at[k - 1, pl.ds(0, self.second)], self.r1(k - 1), me, at(axis, step(axis, k), spot_of[1 - axis]),
                )

        def part_sum(self, j):
            axis = self.axis
            row = step(1 - axis, j)
            mine = self.whole[row, spot_of[0]] if axis == 0 else self.whole[spot_of[1], row]
            total = mine.astype(F32)
            for k in range(1, self.first):
                total = total + self.one[k - 1, row].astype(F32)
            return total

        def middle(self):
            axis = self.axis
            for k in range(1, self.first):
                here = self.one.at[k - 1, pl.ds(0, self.second)]
                landed(here, self.r1(k - 1))
            for j in range(1, self.second):
                self.pair[j - 1] = self.part_sum(j).astype(BF16)
            for j in range(1, self.second):
                start(
                    self.pair.at[j - 1], self.two.at[j - 1], self.r2(j - 1), me, at(axis, spot_of[axis], step(1 - axis, j)),
                )

        def end(self):
            total = self.part_sum(0)
            for j in range(1, self.second):
                here = self.two.at[j - 1]
                landed(here, self.r2(j - 1))
                total = total + self.two[j - 1].astype(F32)
            return total

    halves = all(n % 2 == 0 for n in extent)
    parity = lax.rem(spot_of[0] + spot_of[1], 2) if halves else 0
    taken = pl.ds(2 * parity, 2) if halves else pl.ds(0, 4)

    def latent_pieces(block):
        return (latent.at[block, taken], turned.at[block])

    def latent_send(d):
        target = facing(d)[0] * 2 + core
        for i, here in enumerate(latent_pieces(me)):
            start(here, here, kz_recv.at[d - 1, i], target, part)

    def latent_pass(d):
        block = facing(d)[1] * 2 + core
        for i, here in enumerate(latent_pieces(block)):
            landed(here, kz_recv.at[d - 1, i])
        if halves:
            for a in range(2):
                here = latent.at[block, 2 * parity + a]
                target = at(a, step(a, 1), spot_of[1 - a])
                start(here, here, kx_recv.at[d - 1, a], me, target)
        for i, here in enumerate(latent_pieces(block)):
            start(here, here, kc_recv.at[d - 1, i], twin, part)

    def latent_rest(d):
        if halves:
            for a in range(2):
                here = latent.at[facing(d)[1] * 2 + core, 2 * (1 - parity) + a]
                landed(here, kx_recv.at[d - 1, a])
                start(here, here, kc_recv.at[d - 1, 2 + a], twin, part)

    def latent_twin(d):
        if d == 0:
            for i, whole in enumerate((latent, turned)):
                here = whole.at[twin]
                landed(here, ko_recv.at[i])
            return
        block = facing(d)[1] * 2 + 1 - core
        for i, here in enumerate(latent_pieces(block)):
            landed(here, kc_recv.at[d - 1, i])
        if halves:
            for a in range(2):
                here = latent.at[block, 2 * (1 - parity) + a]
                landed(here, kc_recv.at[d - 1, 2 + a])

    def row_send(d, cores=(0, 1)):
        for c in cores:
            target = facing(d)[0] * 2 + c
            start(send_rows.at[target], rows.at[me, :, columns(part)], dz_recv.at[d - 1, core], target, part)

    def row_share(d, c):
        block = facing(d)[1] * 2 + c
        return Share(
            lambda index: rows.at[block, :, columns(index)],
            lambda n: dt_recv.at[d - 1, c, n], c,
        )

    def row_direct(d, cores=(0, 1)):
        for c in cores:
            here = rows.at[facing(d)[1] * 2 + c, :, columns(part)]
            landed(here, dz_recv.at[d - 1, c])
            row_share(d, c).direct()

    def row_relay(d):
        for c in range(2):
            row_share(d, c).relay()

    def row_finish(d):
        if d == 0:
            here = rows.at[twin]
            landed(here, do_recv.at[0])
            return
        for c in range(2):
            row_share(d, c).finish()

    def row_sum(d, c):
        block = facing(d)[1] * 2 + c
        return Sum(
            part_rows.at[block], first_rows.at[block], pair_rows.at[block], second_rows.at[block],
            lambda n: p_recv.at[d, c, n], lambda n: q_recv.at[d, c, n], c,
        )

    block = min(256, v_gate.shape[1])

    def run_expert(d):
        first = facing(d)[1] * 2
        arrived = rows[pl.ds(first, 2)].reshape(2 * slots, width)
        for j in range(v_gate.shape[1] // block):
            units = slice(j * block, (j + 1) * block)
            gate = dot(arrived, v_gate[:, units])
            up = dot(arrived, v_up[:, units])
            hidden[:, units] = (gate / (1.0 + jnp.exp(-gate)) * up).astype(BF16)
        if d == 0:
            loads[3].wait()
        for n in range(tp_size):
            result = dot(hidden[...], v_down[:, n * features : (n + 1) * features]).astype(BF16)
            part_rows[pl.ds(first, 2), n // extent[0], n % extent[0]] = result.reshape(2, slots, features)

    def sum_begin(d):
        for c in range(2):
            row_sum(d, c).begin()

    def sum_middle(d):
        for c in range(2):
            row_sum(d, c).middle()

    def sum_end(d):
        other = facing(d)[1]
        for c in range(2):
            reduced[other * 2 + c] = row_sum(d, c).end().astype(BF16)
        if d == 0:
            comb[me] = reduced[me]
            start(reduced.at[twin], comb.at[me], r_recv.at[0, 0], twin, part)
            return
        for c in range(2):
            source = other * 2 + c
            start(reduced.at[source], comb.at[me], r_recv.at[d, core], source, part)

    def mix_sum(h):
        return Sum(
            mix_part.at[h], mix_first.at[h], mix_pair.at[h], mix_second.at[h],
            lambda n: m_recv.at[h, n], lambda n: n_recv.at[h, n], h,
        )

    def queries():
        for load in small[9:] + loads[:1]:
            load.wait()
        q_normed = rms_scale(q_lat[...], q_gain[...]).astype(BF16)
        query = dot(q_normed, v_query[...])
        for h in range(heads):
            base = h * (NOPE + ROPE)
            qcat[h, :, :NOPE] = query[:, base : base + NOPE].astype(BF16)
            turn = query[:, base + NOPE : base + NOPE + ROPE].astype(BF16)
            qcat[h, :, NOPE:] = rotate(turn, spun[0], 1)

    def make_keys(d):
        first = facing(d)[1] * 2
        span = 2 * count
        tokens_in = pl.ds(pl.multiple_of(first * count, span), span)
        some = latent[pl.ds(first, 2)].reshape(span, rank)
        keys = dot(some, v_key[...]).astype(BF16)
        vals[tokens_in, :] = dot(some, v_value[...]).astype(BF16)
        both = turned[pl.ds(first, 2)]
        low = lax.broadcasted_iota(jnp.int32, both.shape, 2) < ROPE
        none = jnp.zeros_like(both)
        spread = jnp.concatenate([jnp.where(low, both, none), jnp.where(low, none, both)], 1)
        for h in range(heads):
            kcat[h, tokens_in, :NOPE] = keys[:, h * NOPE : (h + 1) * NOPE]
            kcat[h, tokens_in, NOPE:] = spread.reshape(span, 128)

    def attend(h):
        factor = (NOPE + ROPE) ** (-0.5)
        score = lax.dot_general(
            qcat[h], kcat[h], (((1,), (1,)), ((), ())), preferred_element_type=F32
        ) * factor
        peak = jnp.max(score, -1, keepdims=True)
        weights = jnp.exp(score - peak)
        total = jnp.sum(weights, -1, keepdims=True)
        summed = dot(weights.astype(BF16), vals[:, h * VDIM : (h + 1) * VDIM])
        attended[:, h * VDIM : (h + 1) * VDIM] = (summed / total).astype(BF16)

    def make_mix():
        loads[6].wait()
        half = width // 2
        for h in range(2):
            result = dot(attended[...], v_mix[:, h * half : (h + 1) * half]).astype(BF16)
            mix_part[h] = result.reshape(mix_part.shape[1:])

    def mix_begin():
        for h in range(2):
            mix_sum(h).begin()

    def mix_middle():
        for h in range(2):
            mix_sum(h).middle()

    def mix_end():
        half = width // 2
        for h in range(2):
            mixed[:, h * half : (h + 1) * half] = mix_sum(h).end().astype(BF16)
        outs[0].start()

    for d in order[:1]:
        row_send(d)
    prepare_latents()
    for load in loads[1:3]:
        load.wait()
    row_finish(0)
    run_expert(0)
    sum_begin(0)
    queries()
    for load in loads[4:6]:
        load.wait()
    latent_twin(0)
    make_keys(0)
    for d in order[:1]:
        row_direct(d)
    for d in order[1:]:
        row_send(d)
    sum_middle(0)
    for d in order[:1]:
        row_relay(d)
    for d in order:
        latent_send(d)
    for d in order[1:2]:
        row_direct(d)
    groups = [0] + order
    last = len(order) - 1
    pending = [functools.partial(attend, h) for h in range(heads)]
    ended = 0

    def some_heads(number):
        for work in pending[:number]:
            work()
        del pending[:number]

    for i, d in enumerate(order):
        row_finish(d)
        if i + 2 <= last:
            row_direct(order[i + 2])
        if 0 < i < last:
            row_relay(order[i + 1])
        run_expert(d)
        if i == 0 and last > 0:
            row_relay(order[1])
        sum_begin(d)
        if i == max(0, last - 2):
            for e in order:
                latent_pass(e)
        if i == 1:
            sum_middle(groups[1])
            sum_end(0)
            ended = 1
        if i == max(0, last - 1):
            for e in order:
                latent_rest(e)
            for e in order:
                latent_twin(e)
                make_keys(e)
        if i == last:
            some_heads(1)
        if i > 1:
            sum_middle(groups[i])
            some_heads(1)
            while ended < i:
                sum_end(groups[ended])
                ended += 1
    some_heads(heads)
    make_mix()
    for d in groups[-1:]:
        sum_middle(d)
    mix_begin()
    for d in groups[ended:]:
        sum_end(d)
    mix_middle()
    mix_end()

    here = comb.at[twin]
    landed(here, r_recv.at[0, 0])
    for d in order:
        for c in range(2):
            here = comb.at[facing(d)[0] * 2 + c]
            landed(here, r_recv.at[d, c])
    back = comb[...].reshape(ep_size * slots, features)
    seat = lax.broadcasted_iota(jnp.int32, (tokens, ep_size * slots), 1).astype(F32)
    result = jnp.zeros((tokens, features), F32)
    for k in range(choose):
        pick = jnp.where(seat == facts[:, k : k + 1], 1.0, 0.0).astype(BF16)
        result = result + dot(pick, back) * facts[:, choose + k : choose + k + 1]
    expert_out[...] = result.astype(BF16)
    outs[1].start()
    for copy in waits[-pool.shape[0] :]:
        copy.wait_send()
    for out in outs:
        out.wait()


def hand_over(mixed_in, expert_in, mixed, expert_out):
    mixed[...] = mixed_in[: mixed.shape[0]]
    expert_out[...] = expert_in[...]


def body(
    q_latent,
    kv_latent,
    rope_key,
    q_gain,
    kv_gain,
    w_query,
    w_key,
    w_value,
    w_mix_out,
    expert_in,
    norm_gain,
    routes,
    route_scores,
    w_gate,
    w_up,
    w_down,
):
    ep_size, tp_size = lax.axis_size("ep"), lax.axis_size("tp")
    levels = ep_size // 2
    tokens, width = expert_in.shape
    count = kv_latent.shape[0]
    choose = routes.shape[1]
    slots = 2 * choose * tokens // ep_size
    heads = w_query.shape[1] // (NOPE + ROPE)
    features = width // tp_size
    units = w_gate.shape[2]
    mine = count // tp_size
    padded = -(-mine // 16) * 16
    queries = padded * tp_size
    narrow = math.isqrt(tp_size)
    while tp_size % narrow:
        narrow -= 1
    extent = (tp_size // narrow, narrow)
    most = max(extent)
    ahead = max(1, most - 1)
    away = max(1, levels - 1)
    wing = width // 2

    lane = np.arange(128) % (ROPE // 2)
    inverse = np.float32(rope_base) ** (-(2 * lane).astype(np.float32) / np.float32(ROPE))

    def turns(positions):
        phase = positions[:, None].astype(np.float64) * inverse[None, :].astype(np.float64)
        return np.concatenate([np.cos(phase), np.sin(phase)], 1).astype(np.float32)

    near_angle = turns(np.arange(count))
    if padded != mine:
        spread = np.pad(near_angle.reshape(tp_size, mine, 256), ((0, 0), (0, padded - mine), (0, 0)))
        near_angle = np.concatenate([near_angle, spread.reshape(queries, 256)], 0)
    far_angle = turns(np.arange(ep_size) * count)[:, None, :]

    def pad_rows(values):
        if padded == mine:
            return values
        values = values.reshape(tp_size, mine, values.shape[1])
        return jnp.pad(values, ((0, 0), (0, padded - mine), (0, 0))).reshape(queries, -1)

    dma = pltpu.SemaphoreType.DMA
    vmem = pl.BlockSpec(memory_space=pltpu.VMEM)
    far = pl.BlockSpec(memory_space=pl.ANY)
    small = (
        pad_rows(q_latent), kv_latent, rope_key.T, q_gain[None, :], kv_gain[None, :],
        jnp.asarray(near_angle), jnp.asarray(far_angle), expert_in, norm_gain[None, :], routes.T, route_scores.T,
    )
    mixed, expert_out = pl.pallas_call(
        functools.partial(layer_kernel, (ep_size, tp_size, slots, choose, heads, extent)),
        out_shape=(
            jax.ShapeDtypeStruct((padded, width), BF16),
            jax.ShapeDtypeStruct((tokens, features), BF16),
        ),
        in_specs=[far] * 18,
        out_specs=(far, far),
        scratch_shapes=[
            pltpu.VMEM((padded, width), BF16),
            pltpu.VMEM((tokens, features), BF16),
            *[pltpu.VMEM(value.shape, value.dtype) for value in small],
            pltpu.VMEM(w_query.shape, BF16),
            pltpu.VMEM(w_key.shape, BF16),
            pltpu.VMEM(w_value.shape, BF16),
            pltpu.VMEM(w_mix_out.shape, BF16),
            pltpu.VMEM((width, units), BF16),
            pltpu.VMEM((width, units), BF16),
            pltpu.VMEM((units, width), BF16),
            pltpu.VMEM((ep_size, 4, count // 4, kv_latent.shape[1]), BF16),
            pltpu.VMEM((ep_size, count // 2, 128), BF16),
            pltpu.VMEM((heads, ep_size * count, NOPE + 128), BF16),
            pltpu.VMEM((ep_size * count, heads * VDIM), BF16),
            pltpu.VMEM((heads, queries, NOPE + 128), BF16),
            pltpu.VMEM((queries, heads * VDIM), BF16),
            pltpu.VMEM((2, extent[1], extent[0], padded, wing), BF16),
            pltpu.VMEM((2, ahead, most, padded, wing), BF16),
            pltpu.VMEM((2, ahead, padded, wing), BF16),
            pltpu.VMEM((2, ahead, padded, wing), BF16),
            pltpu.VMEM((tokens, width), BF16),
            pltpu.VMEM((ep_size * slots, tokens), BF16),
            pltpu.VMEM((tokens, 128), F32),
            pltpu.VMEM((ep_size, slots, features), BF16),
            pltpu.VMEM((slots, width), BF16),
            pltpu.VMEM((ep_size, slots, width), BF16),
            pltpu.VMEM((2 * slots, units), BF16),
            pltpu.VMEM((ep_size, extent[1], extent[0], slots, features), BF16),
            pltpu.VMEM((ep_size, ahead, most, slots, features), BF16),
            pltpu.VMEM((ep_size, ahead, slots, features), BF16),
            pltpu.VMEM((ep_size, ahead, slots, features), BF16),
            pltpu.VMEM((ep_size, slots, features), BF16),
            pltpu.VMEM((ep_size, slots, features), BF16),
            dma((7,)), dma((11,)), dma((32,)),
            dma((away, 2)), dma((away, 2)), dma((away, 4)), dma((2,)),
            dma((away, 2)), dma((away, 2, max(1, tp_size - 1))), dma((1,)),
            dma((levels, 2, ahead)), dma((levels, 2, ahead)), dma((levels, 2)),
            dma((2, ahead)), dma((2, ahead)),
        ],
        compiler_params=pltpu.CompilerParams(
            collective_id=0, has_side_effects=True, vmem_limit_bytes=60 * 1024 * 1024
        ),
    )(
        *small,
        w_query, w_key, w_value, w_mix_out, w_gate[0], w_up[0], w_down[0],
    )
    return pl.pallas_call(
        hand_over,
        out_shape=(
            jax.ShapeDtypeStruct((mine, width), BF16),
            jax.ShapeDtypeStruct((tokens, features), BF16),
        ),
        in_specs=[vmem] * 2,
        out_specs=(vmem, vmem),
    )(mixed, expert_out)


def solution(mesh):
    in_specs = (
        P("ep", None),
        P("ep", None),
        P("ep", None),
        P(),
        P(),
        P(None, "tp"),
        P(None, "tp"),
        P(None, "tp"),
        P("tp", None),
        P("ep", None),
        P(),
        P("ep", None),
        P("ep", None),
        P("ep", None, "tp"),
        P("ep", None, "tp"),
        P("ep", "tp", None),
    )
    out_specs = (P(("ep", "tp"), None), P("ep", "tp"))
    return jax.shard_map(body, mesh=mesh, in_specs=in_specs, out_specs=out_specs, check_vma=False)
```

```python
import functools
import math

import jax
import jax.numpy as jnp
import numpy as np
from jax import lax
from jax.experimental import pallas as pl
from jax.experimental.pallas import tpu as pltpu
from jax.sharding import PartitionSpec as P

NOPE = 128
ROPE = 64
VDIM = 128

eps_norm = 1e-05
rope_base = 10000.0

MESH = pl.DeviceIdType.MESH
F32 = jnp.float32
BF16 = jnp.bfloat16


def remote(src, dst, send, recv, ep, tp):
    return pltpu.make_async_remote_copy(
        src_ref=src, dst_ref=dst, send_sem=send, recv_sem=recv, device_id=(ep, tp), device_id_type=MESH
    )


def dot(left, right):
    return jnp.dot(left, right, preferred_element_type=F32)


def rms_scale(values, gain):
    wide = values.astype(F32)
    return wide * lax.rsqrt(jnp.mean(wide * wide, -1, keepdims=True) + eps_norm) * gain


def rotate(values, angles, axis):
    source = lax.broadcasted_iota(jnp.int32, (ROPE, 256), 0)
    lane = lax.broadcasted_iota(jnp.int32, (ROPE, 256), 1)
    same = (lane < 128) & (source == lane % ROPE)
    turned = (lane >= 128) & (source == (lane + ROPE // 2) % ROPE)
    spread = jnp.where(same | turned, 1.0, 0.0).astype(BF16)
    wide = lax.dot_general(
        values, spread, (((axis,), (0,)), ((), ())), preferred_element_type=F32
    )
    return (wide[:, :128] * angles[0] + wide[:, 128:] * angles[1]).astype(BF16)


def layer_kernel(
    sizes,
    h_q_lat, h_kv_lat, h_rope_key, h_q_gain, h_kv_gain, h_near_angle, h_far_angle, h_expert_in, h_norm_gain, h_routes, h_scores,
    w_query, w_key, w_value, w_mix, w_gate, w_up, w_down,
    mixed_far, expert_far,
    mixed, expert_out, q_lat, kv_lat, rope_key, q_gain, kv_gain, near_angle, far_angle, expert_in, norm_gain, routes, scores,
    v_query, v_key, v_value, v_mix, v_gate, v_up, v_down,
    latent, turned, kcat, vals, qcat, attended, mix_part, mix_first, mix_pair, mix_second,
    normed, place, facts, send_rows, twin_rows, rows, hidden, part_rows, first_rows, pair_rows, second_rows,
    reduced, comb,
    w_sem, i_sem, pool, kz_recv, kx_recv, kc_recv, ko_recv, dz_recv, dt_recv, do_recv, p_recv, q_recv, r_recv, m_recv, n_recv,
):
    ep_size, tp_size, slots, choose, heads, extent = sizes
    levels = ep_size // 2
    me = lax.axis_index("ep")
    part = lax.axis_index("tp")
    level, core = me // 2, me % 2
    twin = level * 2 + 1 - core
    spot_of = (part % extent[0], part // extent[0])
    tokens, width = expert_in.shape
    features = width // tp_size
    count, rank = kv_lat.shape
    waits = []
    spun = [None]

    def start(src, dst, recv, ep, tp):
        slot = len(waits) % pool.shape[0]
        if len(waits) >= pool.shape[0]:
            waits[len(waits) - pool.shape[0]].wait_send()
        copy = remote(src, dst, pool.at[slot], recv, ep, tp)
        copy.start()
        waits.append(copy)

    def landed(here, recv):
        remote(here, here, pool.at[0], recv, twin, part).wait_recv()

    def columns(index):
        return pl.ds(pl.multiple_of(index * features, features), features)

    def step(axis, k):
        return lax.rem(spot_of[axis] + k, extent[axis])

    def at(axis, first, second):
        return second * extent[0] + first if axis == 0 else first * extent[0] + second

    def facing(d):
        if levels & (levels - 1):
            return lax.rem(level + d, levels), lax.rem(level - d + levels, levels)
        other = level
        bit = 1
        while bit < levels:
            if d & bit:
                other = other + bit * (1 - 2 * (level // bit % 2))
            bit *= 2
        return other, other

    small = [
        pltpu.make_async_copy(src, dst, i_sem.at[i])
        for i, (src, dst) in enumerate((
            (h_kv_lat, kv_lat), (h_rope_key, rope_key), (h_kv_gain, kv_gain), (h_near_angle, near_angle),
            (h_far_angle, far_angle), (h_routes, routes), (h_scores, scores), (h_expert_in, expert_in),
            (h_norm_gain, norm_gain), (h_q_lat, q_lat), (h_q_gain, q_gain),
        ))
    ]
    for load in small[5:9] + small[:5] + small[9:]:
        load.start()
    barrier = pltpu.get_barrier_semaphore()
    for d in range(1, ep_size):
        pl.semaphore_signal(
            barrier, inc=1, device_id=(lax.rem(me + d, ep_size), part), device_id_type=MESH
        )
    for k in range(1, tp_size):
        pl.semaphore_signal(
            barrier, inc=1, device_id=(me, lax.rem(part + k, tp_size)), device_id_type=MESH
        )
    loads = [
        pltpu.make_async_copy(src, dst, w_sem.at[i])
        for i, (src, dst) in enumerate((
            (w_query, v_query), (w_gate, v_gate), (w_up, v_up), (w_down, v_down),
            (w_key, v_key), (w_value, v_value), (w_mix, v_mix),
        ))
    ]
    for i in (4, 5, 0, 1):
        loads[i].start()

    for load in small[5:9]:
        load.wait()
    for i in (2, 3, 6):
        loads[i].start()

    named = routes[...]
    experts = max(8, ep_size)
    expert = lax.broadcasted_iota(jnp.int32, (experts, tokens), 0)
    member = [expert == named[k : k + 1, :] for k in range(choose)]
    any_member = member[0]
    for k in range(1, choose):
        any_member = any_member | member[k]
    earlier = lax.broadcasted_iota(jnp.int32, (tokens, tokens), 0) < lax.broadcasted_iota(
        jnp.int32, (tokens, tokens), 1
    )
    before = dot(
        jnp.where(any_member, 1.0, 0.0).astype(BF16), jnp.where(earlier, 1.0, 0.0).astype(BF16)
    )
    spot = before + (expert * slots).astype(F32)
    targets = [
        jnp.sum(jnp.where(member[k], spot, 0.0), 0, keepdims=True) for k in range(choose)
    ]
    score = scores[...]
    shares = score / jnp.sum(score, 0, keepdims=True)
    known = jnp.concatenate(targets + [shares], 0)
    known = jnp.concatenate([known, jnp.zeros((128 - 2 * choose, tokens), F32)], 0)
    facts[...] = jnp.transpose(known)
    seat = lax.broadcasted_iota(jnp.int32, (ep_size * slots, tokens), 0).astype(F32)
    chosen = seat == targets[0]
    for k in range(1, choose):
        chosen = chosen | (seat == targets[k])
    place[...] = jnp.where(chosen, 1.0, 0.0).astype(BF16)

    wide = expert_in[...].astype(F32)
    centered = wide - jnp.mean(wide, -1, keepdims=True)
    normed[...] = (
        centered
        * lax.rsqrt(jnp.mean(centered * centered, -1, keepdims=True) + eps_norm)
        * norm_gain[...]
    ).astype(BF16)


    def seats(index):
        return place[pl.ds(pl.multiple_of(index * slots, slots), slots), :]

    send_rows[...] = dot(place[...], normed[:, columns(part)]).astype(BF16).reshape(send_rows.shape)
    twin_rows[...] = dot(seats(twin), normed[...]).astype(BF16)
    rows[me] = dot(seats(me), normed[...]).astype(BF16)

    pl.semaphore_wait(barrier, ep_size + tp_size - 2)

    outs = [
        pltpu.make_async_copy(mixed, mixed_far, w_sem.at[0]),
        pltpu.make_async_copy(expert_out, expert_far, w_sem.at[1]),
    ]
    near = list(range(1, levels))
    order = near[::-1]
    start(twin_rows, rows.at[me], do_recv.at[0], twin, part)

    def prepare_latents():
        for load in small[:5]:
            load.wait()
        block_cosine = far_angle[me][:, :128]
        block_sine = far_angle[me][:, 128:]

        def turn_by(first, last):
            own_cosine, own_sine = near_angle[first:last, :128], near_angle[first:last, 128:]
            lane = lax.broadcasted_iota(jnp.int32, own_sine.shape, 1)
            sine = block_sine * own_cosine + block_cosine * own_sine
            return (
                block_cosine * own_cosine - block_sine * own_sine,
                jnp.where(lane % ROPE < ROPE // 2, -sine, sine),
            )

        angles = turn_by(0, count)
        spun[0] = angles if q_lat.shape[0] == count else turn_by(count, count + q_lat.shape[0])
        kv_normed = rms_scale(kv_lat[...], kv_gain[...]).astype(BF16)
        key_turned = rotate(rope_key[...], angles, 0)
        latent[me] = kv_normed.reshape(latent.shape[1:])
        low = lax.broadcasted_iota(jnp.int32, (count // 2, 128), 1) < ROPE
        turned[me] = jnp.where(low, key_turned[: count // 2], key_turned[count // 2 :])
        for i, whole in enumerate((latent, turned)):
            start(whole.at[me], whole.at[me], ko_recv.at[i], twin, part)

    class Share:
        def __init__(self, view, recvs, axis):
            self.view, self.recvs, self.axis = view, recvs, axis
            self.first, self.second = extent[axis], extent[1 - axis]

        def number(self, k, j):
            if j == 0:
                return k - 1
            if k == 0:
                return self.first - 1 + j - 1
            return self.first + self.second - 2 + (k - 1) * (self.second - 1) + j - 1

        def index(self, k, j):
            axis = self.axis
            return at(axis, step(axis, self.first - k if k else 0), step(1 - axis, self.second - j if j else 0))

        def push(self, here, k, j, target):
            number = self.number(k, j)
            start(here, here, self.recvs(number), me, target)

        def arrive(self, k, j):
            number, index = self.number(k, j), self.index(k, j)
            here = self.view(index)
            landed(here, self.recvs(number))
            return here

        def direct(self):
            axis, here = self.axis, self.view(part)
            for k in range(1, self.first):
                self.push(here, k, 0, at(axis, step(axis, k), spot_of[1 - axis]))
            for j in range(1, self.second):
                self.push(here, 0, j, at(axis, spot_of[axis], step(1 - axis, j)))

        def relay(self):
            axis = self.axis
            for k in range(1, self.first):
                here = self.arrive(k, 0)
                for j in range(1, self.second):
                    self.push(here, k, j, at(axis, spot_of[axis], step(1 - axis, j)))

        def finish(self):
            for j in range(1, self.second):
                for k in range(self.first):
                    self.arrive(k, j)

    class Sum:
        def __init__(self, whole, one, pair, two, r1, r2, axis):
            self.whole, self.one, self.pair, self.two = whole, one, pair, two
            self.r1, self.r2, self.axis = r1, r2, axis
            self.first, self.second = extent[axis], extent[1 - axis]

        def strip(self, index):
            return self.whole.at[:, index] if self.axis == 0 else self.whole.at[index]

        def begin(self):
            axis = self.axis
            for k in range(1, self.first):
                start(
                    self.strip(step(axis, k)), self.one.at[k - 1, pl.ds(0, self.second)], self.r1(k - 1), me, at(axis, step(axis, k), spot_of[1 - axis]),
                )

        def part_sum(self, j):
            axis = self.axis
            row = step(1 - axis, j)
            mine = self.whole[row, spot_of[0]] if axis == 0 else self.whole[spot_of[1], row]
            total = mine.astype(F32)
            for k in range(1, self.first):
                total = total + self.one[k - 1, row].astype(F32)
            return total

        def middle(self):
            axis = self.axis
            for k in range(1, self.first):
                here = self.one.at[k - 1, pl.ds(0, self.second)]
                landed(here, self.r1(k - 1))
            for j in range(1, self.second):
                self.pair[j - 1] = self.part_sum(j).astype(BF16)
            for j in range(1, self.second):
                start(
                    self.pair.at[j - 1], self.two.at[j - 1], self.r2(j - 1), me, at(axis, spot_of[axis], step(1 - axis, j)),
                )

        def end(self):
            total = self.part_sum(0)
            for j in range(1, self.second):
                here = self.two.at[j - 1]
                landed(here, self.r2(j - 1))
                total = total + self.two[j - 1].astype(F32)
            return total

    halves = all(n % 2 == 0 for n in extent)
    parity = lax.rem(spot_of[0] + spot_of[1], 2) if halves else 0
    taken = pl.ds(2 * parity, 2) if halves else pl.ds(0, 4)

    def latent_pieces(block):
        return (latent.at[block, taken], turned.at[block])

    def latent_send(d):
        target = facing(d)[0] * 2 + core
        for i, here in enumerate(latent_pieces(me)):
            start(here, here, kz_recv.at[d - 1, i], target, part)

    def latent_pass(d):
        block = facing(d)[1] * 2 + core
        for i, here in enumerate(latent_pieces(block)):
            landed(here, kz_recv.at[d - 1, i])
        if halves:
            for a in range(2):
                here = latent.at[block, 2 * parity + a]
                target = at(a, step(a, 1), spot_of[1 - a])
                start(here, here, kx_recv.at[d - 1, a], me, target)
        for i, here in enumerate(latent_pieces(block)):
            start(here, here, kc_recv.at[d - 1, i], twin, part)

    def latent_rest(d):
        if halves:
            for a in range(2):
                here = latent.at[facing(d)[1] * 2 + core, 2 * (1 - parity) + a]
                landed(here, kx_recv.at[d - 1, a])
                start(here, here, kc_recv.at[d - 1, 2 + a], twin, part)

    def latent_twin(d):
        if d == 0:
            for i, whole in enumerate((latent, turned)):
                here = whole.at[twin]
                landed(here, ko_recv.at[i])
            return
        block = facing(d)[1] * 2 + 1 - core
        for i, here in enumerate(latent_pieces(block)):
            landed(here, kc_recv.at[d - 1, i])
        if halves:
            for a in range(2):
                here = latent.at[block, 2 * (1 - parity) + a]
                landed(here, kc_recv.at[d - 1, 2 + a])

    def row_send(d, cores=(0, 1)):
        for c in cores:
            target = facing(d)[0] * 2 + c
            start(send_rows.at[target], rows.at[me, :, columns(part)], dz_recv.at[d - 1, core], target, part)

    def row_share(d, c):
        block = facing(d)[1] * 2 + c
        return Share(
            lambda index: rows.at[block, :, columns(index)],
            lambda n: dt_recv.at[d - 1, c, n], c,
        )

    def row_direct(d, cores=(0, 1)):
        for c in cores:
            here = rows.at[facing(d)[1] * 2 + c, :, columns(part)]
            landed(here, dz_recv.at[d - 1, c])
            row_share(d, c).direct()

    def row_relay(d):
        for c in range(2):
            row_share(d, c).relay()

    def row_finish(d):
        if d == 0:
            here = rows.at[twin]
            landed(here, do_recv.at[0])
            return
        for c in range(2):
            row_share(d, c).finish()

    def row_sum(d, c):
        block = facing(d)[1] * 2 + c
        return Sum(
            part_rows.at[block], first_rows.at[block], pair_rows.at[block], second_rows.at[block],
            lambda n: p_recv.at[d, c, n], lambda n: q_recv.at[d, c, n], c,
        )

    block = min(512, v_gate.shape[1])

    def run_expert(d):
        first = facing(d)[1] * 2
        arrived = rows[pl.ds(first, 2)].reshape(2 * slots, width)
        for j in range(v_gate.shape[1] // block):
            units = slice(j * block, (j + 1) * block)
            gate = dot(arrived, v_gate[:, units])
            up = dot(arrived, v_up[:, units])
            hidden[:, units] = (gate / (1.0 + jnp.exp(-gate)) * up).astype(BF16)
        if d == 0:
            loads[3].wait()
        for n in range(tp_size):
            result = dot(hidden[...], v_down[:, n * features : (n + 1) * features]).astype(BF16)
            part_rows[pl.ds(first, 2), n // extent[0], n % extent[0]] = result.reshape(2, slots, features)

    def sum_begin(d):
        for c in range(2):
            row_sum(d, c).begin()

    def sum_middle(d):
        for c in range(2):
            row_sum(d, c).middle()

    def sum_end(d):
        other = facing(d)[1]
        for c in range(2):
            reduced[other * 2 + c] = row_sum(d, c).end().astype(BF16)
        if d == 0:
            comb[me] = reduced[me]
            start(reduced.at[twin], comb.at[me], r_recv.at[0, 0], twin, part)
            return
        for c in range(2):
            source = other * 2 + c
            start(reduced.at[source], comb.at[me], r_recv.at[d, core], source, part)

    def mix_sum(h):
        return Sum(
            mix_part.at[h], mix_first.at[h], mix_pair.at[h], mix_second.at[h],
            lambda n: m_recv.at[h, n], lambda n: n_recv.at[h, n], h,
        )

    def queries():
        for load in small[9:] + loads[:1]:
            load.wait()
        q_normed = rms_scale(q_lat[...], q_gain[...]).astype(BF16)
        query = dot(q_normed, v_query[...])
        for h in range(heads):
            base = h * (NOPE + ROPE)
            qcat[h, :, :NOPE] = query[:, base : base + NOPE].astype(BF16)
            turn = query[:, base + NOPE : base + NOPE + ROPE].astype(BF16)
            qcat[h, :, NOPE:] = rotate(turn, spun[0], 1)

    def make_keys(d):
        first = facing(d)[1] * 2
        span = 2 * count
        tokens_in = pl.ds(pl.multiple_of(first * count, span), span)
        some = latent[pl.ds(first, 2)].reshape(span, rank)
        keys = dot(some, v_key[...]).astype(BF16)
        vals[tokens_in, :] = dot(some, v_value[...]).astype(BF16)
        both = turned[pl.ds(first, 2)]
        low = lax.broadcasted_iota(jnp.int32, both.shape, 2) < ROPE
        none = jnp.zeros_like(both)
        spread = jnp.concatenate([jnp.where(low, both, none), jnp.where(low, none, both)], 1)
        for h in range(heads):
            kcat[h, tokens_in, :NOPE] = keys[:, h * NOPE : (h + 1) * NOPE]
            kcat[h, tokens_in, NOPE:] = spread.reshape(span, 128)

    def attend(h):
        factor = (NOPE + ROPE) ** (-0.5)
        score = lax.dot_general(
            qcat[h], kcat[h], (((1,), (1,)), ((), ())), preferred_element_type=F32
        ) * factor
        peak = jnp.max(score, -1, keepdims=True)
        weights = jnp.exp(score - peak)
        total = jnp.sum(weights, -1, keepdims=True)
        summed = dot(weights.astype(BF16), vals[:, h * VDIM : (h + 1) * VDIM])
        attended[:, h * VDIM : (h + 1) * VDIM] = (summed / total).astype(BF16)

    def make_mix():
        loads[6].wait()
        half = width // 2
        for h in range(2):
            result = dot(attended[...], v_mix[:, h * half : (h + 1) * half]).astype(BF16)
            mix_part[h] = result.reshape(mix_part.shape[1:])

    def mix_begin():
        for h in range(2):
            mix_sum(h).begin()

    def mix_middle():
        for h in range(2):
            mix_sum(h).middle()

    def mix_end():
        half = width // 2
        for h in range(2):
            mixed[:, h * half : (h + 1) * half] = mix_sum(h).end().astype(BF16)
        outs[0].start()

    for d in order[:1]:
        row_send(d)
    prepare_latents()
    for load in loads[1:3]:
        load.wait()
    row_finish(0)
    run_expert(0)
    sum_begin(0)
    queries()
    for load in loads[4:6]:
        load.wait()
    latent_twin(0)
    make_keys(0)
    for d in order[:1]:
        row_direct(d)
    for d in order[1:]:
        row_send(d)
    sum_middle(0)
    for d in order[:1]:
        row_relay(d)
    for d in order:
        latent_send(d)
    for d in order[1:2]:
        row_direct(d)
    groups = [0] + order
    last = len(order) - 1
    pending = [functools.partial(attend, h) for h in range(heads)]
    ended = 0

    def some_heads(number):
        for work in pending[:number]:
            work()
        del pending[:number]

    for i, d in enumerate(order):
        row_finish(d)
        if i + 2 <= last:
            row_direct(order[i + 2])
        if 0 < i < last:
            row_relay(order[i + 1])
        run_expert(d)
        if i == 0 and last > 0:
            row_relay(order[1])
        if i == max(0, last - 2):
            for e in order:
                latent_pass(e)
        sum_begin(d)
        if i == max(0, last - 1):
            for e in order:
                latent_rest(e)
            for e in order:
                latent_twin(e)
                make_keys(e)
        if i == 1:
            sum_middle(groups[1])
            sum_end(0)
            ended = 1
            some_heads(1)
        if i == last:
            some_heads(1)
        if i > 1:
            sum_middle(groups[i])
            some_heads(1)
            while ended < i:
                sum_end(groups[ended])
                ended += 1
    some_heads(heads)
    make_mix()
    for d in groups[-1:]:
        sum_middle(d)
    mix_begin()
    for d in groups[ended:]:
        sum_end(d)
    mix_middle()
    mix_end()

    here = comb.at[twin]
    landed(here, r_recv.at[0, 0])
    for d in order:
        for c in range(2):
            here = comb.at[facing(d)[0] * 2 + c]
            landed(here, r_recv.at[d, c])
    back = comb[...].reshape(ep_size * slots, features)
    seat = lax.broadcasted_iota(jnp.int32, (tokens, ep_size * slots), 1).astype(F32)
    result = jnp.zeros((tokens, features), F32)
    for k in range(choose):
        pick = jnp.where(seat == facts[:, k : k + 1], 1.0, 0.0).astype(BF16)
        result = result + dot(pick, back) * facts[:, choose + k : choose + k + 1]
    expert_out[...] = result.astype(BF16)
    outs[1].start()
    for copy in waits[-pool.shape[0] :]:
        copy.wait_send()
    for out in outs:
        out.wait()


def hand_over(mixed_in, expert_in, mixed, expert_out):
    mixed[...] = mixed_in[: mixed.shape[0]]
    expert_out[...] = expert_in[...]


def body(
    q_latent,
    kv_latent,
    rope_key,
    q_gain,
    kv_gain,
    w_query,
    w_key,
    w_value,
    w_mix_out,
    expert_in,
    norm_gain,
    routes,
    route_scores,
    w_gate,
    w_up,
    w_down,
):
    ep_size, tp_size = lax.axis_size("ep"), lax.axis_size("tp")
    levels = ep_size // 2
    tokens, width = expert_in.shape
    count = kv_latent.shape[0]
    choose = routes.shape[1]
    slots = 2 * choose * tokens // ep_size
    heads = w_query.shape[1] // (NOPE + ROPE)
    features = width // tp_size
    units = w_gate.shape[2]
    mine = count // tp_size
    padded = -(-mine // 16) * 16
    queries = padded * tp_size
    narrow = math.isqrt(tp_size)
    while tp_size % narrow:
        narrow -= 1
    extent = (tp_size // narrow, narrow)
    most = max(extent)
    ahead = max(1, most - 1)
    away = max(1, levels - 1)
    wing = width // 2

    lane = np.arange(128) % (ROPE // 2)
    inverse = np.float32(rope_base) ** (-(2 * lane).astype(np.float32) / np.float32(ROPE))

    def turns(positions):
        phase = positions[:, None].astype(np.float64) * inverse[None, :].astype(np.float64)
        return np.concatenate([np.cos(phase), np.sin(phase)], 1).astype(np.float32)

    near_angle = turns(np.arange(count))
    if padded != mine:
        spread = np.pad(near_angle.reshape(tp_size, mine, 256), ((0, 0), (0, padded - mine), (0, 0)))
        near_angle = np.concatenate([near_angle, spread.reshape(queries, 256)], 0)
    far_angle = turns(np.arange(ep_size) * count)[:, None, :]

    def pad_rows(values):
        if padded == mine:
            return values
        values = values.reshape(tp_size, mine, values.shape[1])
        return jnp.pad(values, ((0, 0), (0, padded - mine), (0, 0))).reshape(queries, -1)

    dma = pltpu.SemaphoreType.DMA
    vmem = pl.BlockSpec(memory_space=pltpu.VMEM)
    far = pl.BlockSpec(memory_space=pl.ANY)
    small = (
        pad_rows(q_latent), kv_latent, rope_key.T, q_gain[None, :], kv_gain[None, :],
        jnp.asarray(near_angle), jnp.asarray(far_angle), expert_in, norm_gain[None, :], routes.T, route_scores.T,
    )
    mixed, expert_out = pl.pallas_call(
        functools.partial(layer_kernel, (ep_size, tp_size, slots, choose, heads, extent)),
        out_shape=(
            jax.ShapeDtypeStruct((padded, width), BF16),
            jax.ShapeDtypeStruct((tokens, features), BF16),
        ),
        in_specs=[far] * 18,
        out_specs=(far, far),
        scratch_shapes=[
            pltpu.VMEM((padded, width), BF16),
            pltpu.VMEM((tokens, features), BF16),
            *[pltpu.VMEM(value.shape, value.dtype) for value in small],
            pltpu.VMEM(w_query.shape, BF16),
            pltpu.VMEM(w_key.shape, BF16),
            pltpu.VMEM(w_value.shape, BF16),
            pltpu.VMEM(w_mix_out.shape, BF16),
            pltpu.VMEM((width, units), BF16),
            pltpu.VMEM((width, units), BF16),
            pltpu.VMEM((units, width), BF16),
            pltpu.VMEM((ep_size, 4, count // 4, kv_latent.shape[1]), BF16),
            pltpu.VMEM((ep_size, count // 2, 128), BF16),
            pltpu.VMEM((heads, ep_size * count, NOPE + 128), BF16),
            pltpu.VMEM((ep_size * count, heads * VDIM), BF16),
            pltpu.VMEM((heads, queries, NOPE + 128), BF16),
            pltpu.VMEM((queries, heads * VDIM), BF16),
            pltpu.VMEM((2, extent[1], extent[0], padded, wing), BF16),
            pltpu.VMEM((2, ahead, most, padded, wing), BF16),
            pltpu.VMEM((2, ahead, padded, wing), BF16),
            pltpu.VMEM((2, ahead, padded, wing), BF16),
            pltpu.VMEM((tokens, width), BF16),
            pltpu.VMEM((ep_size * slots, tokens), BF16),
            pltpu.VMEM((tokens, 128), F32),
            pltpu.VMEM((ep_size, slots, features), BF16),
            pltpu.VMEM((slots, width), BF16),
            pltpu.VMEM((ep_size, slots, width), BF16),
            pltpu.VMEM((2 * slots, units), BF16),
            pltpu.VMEM((ep_size, extent[1], extent[0], slots, features), BF16),
            pltpu.VMEM((ep_size, ahead, most, slots, features), BF16),
            pltpu.VMEM((ep_size, ahead, slots, features), BF16),
            pltpu.VMEM((ep_size, ahead, slots, features), BF16),
            pltpu.VMEM((ep_size, slots, features), BF16),
            pltpu.VMEM((ep_size, slots, features), BF16),
            dma((7,)), dma((11,)), dma((20,)),
            dma((away, 2)), dma((away, 2)), dma((away, 4)), dma((2,)),
            dma((away, 2)), dma((away, 2, max(1, tp_size - 1))), dma((1,)),
            dma((levels, 2, ahead)), dma((levels, 2, ahead)), dma((levels, 2)),
            dma((2, ahead)), dma((2, ahead)),
        ],
        compiler_params=pltpu.CompilerParams(
            collective_id=0, has_side_effects=True, vmem_limit_bytes=60 * 1024 * 1024
        ),
    )(
        *small,
        w_query, w_key, w_value, w_mix_out, w_gate[0], w_up[0], w_down[0],
    )
    return pl.pallas_call(
        hand_over,
        out_shape=(
            jax.ShapeDtypeStruct((mine, width), BF16),
            jax.ShapeDtypeStruct((tokens, features), BF16),
        ),
        in_specs=[vmem] * 2,
        out_specs=(vmem, vmem),
    )(mixed, expert_out)


def solution(mesh):
    in_specs = (
        P("ep", None),
        P("ep", None),
        P("ep", None),
        P(),
        P(),
        P(None, "tp"),
        P(None, "tp"),
        P(None, "tp"),
        P("tp", None),
        P("ep", None),
        P(),
        P("ep", None),
        P("ep", None),
        P("ep", None, "tp"),
        P("ep", None, "tp"),
        P("ep", "tp", None),
    )
    out_specs = (P(("ep", "tp"), None), P("ep", "tp"))
    return jax.shard_map(body, mesh=mesh, in_specs=in_specs, out_specs=out_specs, check_vma=False)
```

```python
import functools
import math

import jax
import jax.numpy as jnp
import numpy as np
from jax import lax
from jax.experimental import pallas as pl
from jax.experimental.pallas import tpu as pltpu
from jax.sharding import PartitionSpec as P

NOPE = 128
ROPE = 64
VDIM = 128

eps_norm = 1e-05
rope_base = 10000.0

MESH = pl.DeviceIdType.MESH
F32 = jnp.float32
BF16 = jnp.bfloat16


def remote(src, dst, send, recv, ep, tp):
    return pltpu.make_async_remote_copy(
        src_ref=src, dst_ref=dst, send_sem=send, recv_sem=recv, device_id=(ep, tp), device_id_type=MESH
    )


def dot(left, right):
    return jnp.dot(left, right, preferred_element_type=F32)


def rms_scale(values, gain):
    wide = values.astype(F32)
    return wide * lax.rsqrt(jnp.mean(wide * wide, -1, keepdims=True) + eps_norm) * gain


def rotate(values, angles, axis):
    source = lax.broadcasted_iota(jnp.int32, (ROPE, 256), 0)
    lane = lax.broadcasted_iota(jnp.int32, (ROPE, 256), 1)
    same = (lane < 128) & (source == lane % ROPE)
    turned = (lane >= 128) & (source == (lane + ROPE // 2) % ROPE)
    spread = jnp.where(same | turned, 1.0, 0.0).astype(BF16)
    wide = lax.dot_general(
        values, spread, (((axis,), (0,)), ((), ())), preferred_element_type=F32
    )
    return (wide[:, :128] * angles[0] + wide[:, 128:] * angles[1]).astype(BF16)


def layer_kernel(
    sizes,
    h_q_lat, h_kv_lat, h_rope_key, h_q_gain, h_kv_gain, h_near_angle, h_far_angle, h_expert_in, h_norm_gain, h_routes, h_scores,
    w_query, w_key, w_value, w_mix, w_gate, w_up, w_down,
    mixed_far, expert_far,
    mixed, expert_out, q_lat, kv_lat, rope_key, q_gain, kv_gain, near_angle, far_angle, expert_in, norm_gain, routes, scores,
    v_query, v_key, v_value, v_mix, v_gate, v_up, v_down,
    latent, turned, kcat, vals, qcat, attended, mix_part, mix_first, mix_pair, mix_second,
    normed, place, facts, send_rows, twin_rows, rows, hidden, part_rows, first_rows, pair_rows, second_rows,
    reduced, comb,
    w_sem, i_sem, pool, kz_recv, kx_recv, kc_recv, ko_recv, dz_recv, dt_recv, do_recv, p_recv, q_recv, r_recv, m_recv, n_recv,
):
    ep_size, tp_size, slots, choose, heads, extent = sizes
    levels = ep_size // 2
    me = lax.axis_index("ep")
    part = lax.axis_index("tp")
    level, core = me // 2, me % 2
    twin = level * 2 + 1 - core
    spot_of = (part % extent[0], part // extent[0])
    tokens, width = expert_in.shape
    features = width // tp_size
    count, rank = kv_lat.shape
    waits = []
    spun = [None]

    def start(src, dst, recv, ep, tp):
        slot = len(waits) % pool.shape[0]
        if len(waits) >= pool.shape[0]:
            waits[len(waits) - pool.shape[0]].wait_send()
        copy = remote(src, dst, pool.at[slot], recv, ep, tp)
        copy.start()
        waits.append(copy)

    def landed(here, recv):
        remote(here, here, pool.at[0], recv, twin, part).wait_recv()

    def columns(index):
        return pl.ds(pl.multiple_of(index * features, features), features)

    def step(axis, k):
        return lax.rem(spot_of[axis] + k, extent[axis])

    def at(axis, first, second):
        return second * extent[0] + first if axis == 0 else first * extent[0] + second

    def facing(d):
        if levels & (levels - 1):
            return lax.rem(level + d, levels), lax.rem(level - d + levels, levels)
        other = level
        bit = 1
        while bit < levels:
            if d & bit:
                other = other + bit * (1 - 2 * (level // bit % 2))
            bit *= 2
        return other, other

    small = [
        pltpu.make_async_copy(src, dst, i_sem.at[i])
        for i, (src, dst) in enumerate((
            (h_kv_lat, kv_lat), (h_rope_key, rope_key), (h_kv_gain, kv_gain), (h_near_angle, near_angle),
            (h_far_angle, far_angle), (h_routes, routes), (h_scores, scores), (h_expert_in, expert_in),
            (h_norm_gain, norm_gain), (h_q_lat, q_lat), (h_q_gain, q_gain),
        ))
    ]
    for load in small[5:9] + small[:5] + small[9:]:
        load.start()
    barrier = pltpu.get_barrier_semaphore()
    for d in range(1, ep_size):
        pl.semaphore_signal(
            barrier, inc=1, device_id=(lax.rem(me + d, ep_size), part), device_id_type=MESH
        )
    for k in range(1, tp_size):
        pl.semaphore_signal(
            barrier, inc=1, device_id=(me, lax.rem(part + k, tp_size)), device_id_type=MESH
        )
    loads = [
        pltpu.make_async_copy(src, dst, w_sem.at[i])
        for i, (src, dst) in enumerate((
            (w_query, v_query), (w_gate, v_gate), (w_up, v_up), (w_down, v_down),
            (w_key, v_key), (w_value, v_value), (w_mix, v_mix),
        ))
    ]
    for i in (4, 5, 0, 1):
        loads[i].start()

    for load in small[5:9]:
        load.wait()
    for i in (2, 3, 6):
        loads[i].start()

    named = routes[...]
    experts = max(8, ep_size)
    expert = lax.broadcasted_iota(jnp.int32, (experts, tokens), 0)
    member = [expert == named[k : k + 1, :] for k in range(choose)]
    any_member = member[0]
    for k in range(1, choose):
        any_member = any_member | member[k]
    earlier = lax.broadcasted_iota(jnp.int32, (tokens, tokens), 0) < lax.broadcasted_iota(
        jnp.int32, (tokens, tokens), 1
    )
    before = dot(
        jnp.where(any_member, 1.0, 0.0).astype(BF16), jnp.where(earlier, 1.0, 0.0).astype(BF16)
    )
    spot = before + (expert * slots).astype(F32)
    targets = [
        jnp.sum(jnp.where(member[k], spot, 0.0), 0, keepdims=True) for k in range(choose)
    ]
    score = scores[...]
    shares = score / jnp.sum(score, 0, keepdims=True)
    known = jnp.concatenate(targets + [shares], 0)
    known = jnp.concatenate([known, jnp.zeros((128 - 2 * choose, tokens), F32)], 0)
    facts[...] = jnp.transpose(known)
    seat = lax.broadcasted_iota(jnp.int32, (ep_size * slots, tokens), 0).astype(F32)
    chosen = seat == targets[0]
    for k in range(1, choose):
        chosen = chosen | (seat == targets[k])
    place[...] = jnp.where(chosen, 1.0, 0.0).astype(BF16)

    wide = expert_in[...].astype(F32)
    centered = wide - jnp.mean(wide, -1, keepdims=True)
    normed[...] = (
        centered
        * lax.rsqrt(jnp.mean(centered * centered, -1, keepdims=True) + eps_norm)
        * norm_gain[...]
    ).astype(BF16)


    def seats(index):
        return place[pl.ds(pl.multiple_of(index * slots, slots), slots), :]

    send_rows[...] = dot(place[...], normed[:, columns(part)]).astype(BF16).reshape(send_rows.shape)
    twin_rows[...] = dot(seats(twin), normed[...]).astype(BF16)
    rows[me] = dot(seats(me), normed[...]).astype(BF16)

    pl.semaphore_wait(barrier, ep_size + tp_size - 2)

    outs = [
        pltpu.make_async_copy(mixed, mixed_far, w_sem.at[0]),
        pltpu.make_async_copy(expert_out, expert_far, w_sem.at[1]),
    ]
    near = list(range(1, levels))
    order = near[::-1]
    start(twin_rows, rows.at[me], do_recv.at[0], twin, part)

    def prepare_latents():
        for load in small[:5]:
            load.wait()
        block_cosine = far_angle[me][:, :128]
        block_sine = far_angle[me][:, 128:]

        def turn_by(first, last):
            own_cosine, own_sine = near_angle[first:last, :128], near_angle[first:last, 128:]
            lane = lax.broadcasted_iota(jnp.int32, own_sine.shape, 1)
            sine = block_sine * own_cosine + block_cosine * own_sine
            return (
                block_cosine * own_cosine - block_sine * own_sine,
                jnp.where(lane % ROPE < ROPE // 2, -sine, sine),
            )

        angles = turn_by(0, count)
        spun[0] = angles if q_lat.shape[0] == count else turn_by(count, count + q_lat.shape[0])
        kv_normed = rms_scale(kv_lat[...], kv_gain[...]).astype(BF16)
        key_turned = rotate(rope_key[...], angles, 0)
        latent[me] = kv_normed.reshape(latent.shape[1:])
        low = lax.broadcasted_iota(jnp.int32, (count // 2, 128), 1) < ROPE
        turned[me] = jnp.where(low, key_turned[: count // 2], key_turned[count // 2 :])
        for i, whole in enumerate((latent, turned)):
            start(whole.at[me], whole.at[me], ko_recv.at[i], twin, part)

    class Share:
        def __init__(self, view, recvs, axis):
            self.view, self.recvs, self.axis = view, recvs, axis
            self.first, self.second = extent[axis], extent[1 - axis]

        def number(self, k, j):
            if j == 0:
                return k - 1
            if k == 0:
                return self.first - 1 + j - 1
            return self.first + self.second - 2 + (k - 1) * (self.second - 1) + j - 1

        def index(self, k, j):
            axis = self.axis
            return at(axis, step(axis, self.first - k if k else 0), step(1 - axis, self.second - j if j else 0))

        def push(self, here, k, j, target):
            number = self.number(k, j)
            start(here, here, self.recvs(number), me, target)

        def arrive(self, k, j):
            number, index = self.number(k, j), self.index(k, j)
            here = self.view(index)
            landed(here, self.recvs(number))
            return here

        def direct(self):
            axis, here = self.axis, self.view(part)
            for k in range(1, self.first):
                self.push(here, k, 0, at(axis, step(axis, k), spot_of[1 - axis]))
            for j in range(1, self.second):
                self.push(here, 0, j, at(axis, spot_of[axis], step(1 - axis, j)))

        def relay(self):
            axis = self.axis
            for k in range(1, self.first):
                here = self.arrive(k, 0)
                for j in range(1, self.second):
                    self.push(here, k, j, at(axis, spot_of[axis], step(1 - axis, j)))

        def finish(self):
            for j in range(1, self.second):
                for k in range(self.first):
                    self.arrive(k, j)

    class Sum:
        def __init__(self, whole, one, pair, two, r1, r2, axis):
            self.whole, self.one, self.pair, self.two = whole, one, pair, two
            self.r1, self.r2, self.axis = r1, r2, axis
            self.first, self.second = extent[axis], extent[1 - axis]

        def strip(self, index):
            return self.whole.at[:, index] if self.axis == 0 else self.whole.at[index]

        def begin(self):
            axis = self.axis
            for k in range(1, self.first):
                start(
                    self.strip(step(axis, k)), self.one.at[k - 1, pl.ds(0, self.second)], self.r1(k - 1), me, at(axis, step(axis, k), spot_of[1 - axis]),
                )

        def part_sum(self, j):
            axis = self.axis
            row = step(1 - axis, j)
            mine = self.whole[row, spot_of[0]] if axis == 0 else self.whole[spot_of[1], row]
            total = mine.astype(F32)
            for k in range(1, self.first):
                total = total + self.one[k - 1, row].astype(F32)
            return total

        def middle(self):
            axis = self.axis
            for k in range(1, self.first):
                here = self.one.at[k - 1, pl.ds(0, self.second)]
                landed(here, self.r1(k - 1))
            for j in range(1, self.second):
                self.pair[j - 1] = self.part_sum(j).astype(BF16)
            for j in range(1, self.second):
                start(
                    self.pair.at[j - 1], self.two.at[j - 1], self.r2(j - 1), me, at(axis, spot_of[axis], step(1 - axis, j)),
                )

        def end(self):
            total = self.part_sum(0)
            for j in range(1, self.second):
                here = self.two.at[j - 1]
                landed(here, self.r2(j - 1))
                total = total + self.two[j - 1].astype(F32)
            return total

    halves = all(n % 2 == 0 for n in extent)
    parity = lax.rem(spot_of[0] + spot_of[1], 2) if halves else 0
    taken = pl.ds(2 * parity, 2) if halves else pl.ds(0, 4)

    def latent_pieces(block):
        return (latent.at[block, taken], turned.at[block])

    def latent_send(d):
        target = facing(d)[0] * 2 + core
        for i, here in enumerate(latent_pieces(me)):
            start(here, here, kz_recv.at[d - 1, i], target, part)

    def latent_pass(d):
        block = facing(d)[1] * 2 + core
        for i, here in enumerate(latent_pieces(block)):
            landed(here, kz_recv.at[d - 1, i])
        if halves:
            for a in range(2):
                here = latent.at[block, 2 * parity + a]
                target = at(a, step(a, 1), spot_of[1 - a])
                start(here, here, kx_recv.at[d - 1, a], me, target)
        for i, here in enumerate(latent_pieces(block)):
            start(here, here, kc_recv.at[d - 1, i], twin, part)

    def latent_rest(d):
        if halves:
            for a in range(2):
                here = latent.at[facing(d)[1] * 2 + core, 2 * (1 - parity) + a]
                landed(here, kx_recv.at[d - 1, a])
                start(here, here, kc_recv.at[d - 1, 2 + a], twin, part)

    def latent_twin(d):
        if d == 0:
            for i, whole in enumerate((latent, turned)):
                here = whole.at[twin]
                landed(here, ko_recv.at[i])
            return
        block = facing(d)[1] * 2 + 1 - core
        for i, here in enumerate(latent_pieces(block)):
            landed(here, kc_recv.at[d - 1, i])
        if halves:
            for a in range(2):
                here = latent.at[block, 2 * (1 - parity) + a]
                landed(here, kc_recv.at[d - 1, 2 + a])

    def row_send(d, cores=(0, 1)):
        for c in cores:
            target = facing(d)[0] * 2 + c
            start(send_rows.at[target], rows.at[me, :, columns(part)], dz_recv.at[d - 1, core], target, part)

    def row_share(d, c):
        block = facing(d)[1] * 2 + c
        return Share(
            lambda index: rows.at[block, :, columns(index)],
            lambda n: dt_recv.at[d - 1, c, n], c,
        )

    def row_direct(d, cores=(0, 1)):
        for c in cores:
            here = rows.at[facing(d)[1] * 2 + c, :, columns(part)]
            landed(here, dz_recv.at[d - 1, c])
            row_share(d, c).direct()

    def row_relay(d):
        for c in range(2):
            row_share(d, c).relay()

    def row_finish(d):
        if d == 0:
            here = rows.at[twin]
            landed(here, do_recv.at[0])
            return
        for c in range(2):
            row_share(d, c).finish()

    def row_sum(d, c):
        block = facing(d)[1] * 2 + c
        return Sum(
            part_rows.at[block], first_rows.at[block], pair_rows.at[block], second_rows.at[block],
            lambda n: p_recv.at[d, c, n], lambda n: q_recv.at[d, c, n], c,
        )

    block = min(512, v_gate.shape[1])

    def run_expert(d):
        first = facing(d)[1] * 2
        arrived = rows[pl.ds(first, 2)].reshape(2 * slots, width)
        for j in range(v_gate.shape[1] // block):
            units = slice(j * block, (j + 1) * block)
            gate = dot(arrived, v_gate[:, units])
            up = dot(arrived, v_up[:, units])
            hidden[:, units] = (gate / (1.0 + jnp.exp(-gate)) * up).astype(BF16)
        if d == 0:
            loads[3].wait()
        for n in range(tp_size):
            result = dot(hidden[...], v_down[:, n * features : (n + 1) * features]).astype(BF16)
            part_rows[pl.ds(first, 2), n // extent[0], n % extent[0]] = result.reshape(2, slots, features)

    def sum_begin(d):
        for c in range(2):
            row_sum(d, c).begin()

    def sum_middle(d):
        for c in range(2):
            row_sum(d, c).middle()

    def sum_end(d):
        other = facing(d)[1]
        for c in range(2):
            reduced[other * 2 + c] = row_sum(d, c).end().astype(BF16)
        if d == 0:
            comb[me] = reduced[me]
            start(reduced.at[twin], comb.at[me], r_recv.at[0, 0], twin, part)
            return
        for c in range(2):
            source = other * 2 + c
            start(reduced.at[source], comb.at[me], r_recv.at[d, core], source, part)

    def mix_sum(h):
        return Sum(
            mix_part.at[h], mix_first.at[h], mix_pair.at[h], mix_second.at[h],
            lambda n: m_recv.at[h, n], lambda n: n_recv.at[h, n], h,
        )

    def queries():
        for load in small[9:] + loads[:1]:
            load.wait()
        q_normed = rms_scale(q_lat[...], q_gain[...]).astype(BF16)
        query = dot(q_normed, v_query[...])
        for h in range(heads):
            base = h * (NOPE + ROPE)
            qcat[h, :, :NOPE] = query[:, base : base + NOPE].astype(BF16)
            turn = query[:, base + NOPE : base + NOPE + ROPE].astype(BF16)
            qcat[h, :, NOPE:] = rotate(turn, spun[0], 1)

    def make_keys(d):
        first = facing(d)[1] * 2
        span = 2 * count
        tokens_in = pl.ds(pl.multiple_of(first * count, span), span)
        some = latent[pl.ds(first, 2)].reshape(span, rank)
        keys = dot(some, v_key[...]).astype(BF16)
        vals[tokens_in, :] = dot(some, v_value[...]).astype(BF16)
        both = turned[pl.ds(first, 2)]
        low = lax.broadcasted_iota(jnp.int32, both.shape, 2) < ROPE
        none = jnp.zeros_like(both)
        spread = jnp.concatenate([jnp.where(low, both, none), jnp.where(low, none, both)], 1)
        for h in range(heads):
            kcat[h, tokens_in, :NOPE] = keys[:, h * NOPE : (h + 1) * NOPE]
            kcat[h, tokens_in, NOPE:] = spread.reshape(span, 128)

    def attend(h):
        factor = (NOPE + ROPE) ** (-0.5)
        score = lax.dot_general(
            qcat[h], kcat[h], (((1,), (1,)), ((), ())), preferred_element_type=F32
        ) * factor
        peak = jnp.max(score, -1, keepdims=True)
        weights = jnp.exp(score - peak)
        total = jnp.sum(weights, -1, keepdims=True)
        summed = dot(weights.astype(BF16), vals[:, h * VDIM : (h + 1) * VDIM])
        attended[:, h * VDIM : (h + 1) * VDIM] = (summed / total).astype(BF16)

    def make_mix():
        loads[6].wait()
        half = width // 2
        for h in range(2):
            result = dot(attended[...], v_mix[:, h * half : (h + 1) * half]).astype(BF16)
            mix_part[h] = result.reshape(mix_part.shape[1:])

    def mix_begin():
        for h in range(2):
            mix_sum(h).begin()

    def mix_middle():
        for h in range(2):
            mix_sum(h).middle()

    def mix_end():
        half = width // 2
        for h in range(2):
            mixed[:, h * half : (h + 1) * half] = mix_sum(h).end().astype(BF16)
        outs[0].start()

    for d in order[:1]:
        row_send(d)
    prepare_latents()
    for load in loads[1:3]:
        load.wait()
    row_finish(0)
    run_expert(0)
    sum_begin(0)
    queries()
    for load in loads[4:6]:
        load.wait()
    latent_twin(0)
    make_keys(0)
    for d in order[:1]:
        row_direct(d)
    for d in order[1:]:
        row_send(d)
    sum_middle(0)
    for d in order[:1]:
        row_relay(d)
    for d in order:
        latent_send(d)
    for d in order[1:2]:
        row_direct(d)
    groups = [0] + order
    last = len(order) - 1
    pending = [functools.partial(attend, h) for h in range(heads)]
    ended = 0

    keyed = []

    def some_heads(number):
        if not keyed:
            return
        for work in pending[:number]:
            work()
        del pending[:number]

    for i, d in enumerate(order):
        row_finish(d)
        if i + 2 <= last:
            row_direct(order[i + 2])
        if 0 < i < last:
            row_relay(order[i + 1])
        run_expert(d)
        if i == 0 and last > 0:
            row_relay(order[1])
        if i == max(0, last - 2):
            for e in order:
                latent_pass(e)
        sum_begin(d)
        if i == max(0, last - 1):
            for e in order:
                latent_rest(e)
            for e in order:
                latent_twin(e)
                make_keys(e)
            keyed.append(True)
        if i == 1:
            sum_middle(groups[1])
            sum_end(0)
            ended = 1
            some_heads(1)
        if i == last:
            some_heads(1)
        if i > 1:
            sum_middle(groups[i])
            some_heads(1)
            while ended < i:
                sum_end(groups[ended])
                ended += 1
    keyed.append(True)
    some_heads(heads)
    make_mix()
    for d in groups[-1:]:
        sum_middle(d)
    mix_begin()
    for d in groups[ended:]:
        sum_end(d)
    mix_middle()
    mix_end()

    here = comb.at[twin]
    landed(here, r_recv.at[0, 0])
    for d in order:
        for c in range(2):
            here = comb.at[facing(d)[0] * 2 + c]
            landed(here, r_recv.at[d, c])
    back = comb[...].reshape(ep_size * slots, features)
    seat = lax.broadcasted_iota(jnp.int32, (tokens, ep_size * slots), 1).astype(F32)
    result = jnp.zeros((tokens, features), F32)
    for k in range(choose):
        pick = jnp.where(seat == facts[:, k : k + 1], 1.0, 0.0).astype(BF16)
        result = result + dot(pick, back) * facts[:, choose + k : choose + k + 1]
    expert_out[...] = result.astype(BF16)
    outs[1].start()
    for copy in waits[-pool.shape[0] :]:
        copy.wait_send()
    for out in outs:
        out.wait()


def hand_over(mixed_in, expert_in, mixed, expert_out):
    mixed[...] = mixed_in[: mixed.shape[0]]
    expert_out[...] = expert_in[...]


def body(
    q_latent,
    kv_latent,
    rope_key,
    q_gain,
    kv_gain,
    w_query,
    w_key,
    w_value,
    w_mix_out,
    expert_in,
    norm_gain,
    routes,
    route_scores,
    w_gate,
    w_up,
    w_down,
):
    ep_size, tp_size = lax.axis_size("ep"), lax.axis_size("tp")
    levels = ep_size // 2
    tokens, width = expert_in.shape
    count = kv_latent.shape[0]
    choose = routes.shape[1]
    slots = 2 * choose * tokens // ep_size
    heads = w_query.shape[1] // (NOPE + ROPE)
    features = width // tp_size
    units = w_gate.shape[2]
    mine = count // tp_size
    padded = -(-mine // 16) * 16
    queries = padded * tp_size
    narrow = math.isqrt(tp_size)
    while tp_size % narrow:
        narrow -= 1
    extent = (tp_size // narrow, narrow)
    most = max(extent)
    ahead = max(1, most - 1)
    away = max(1, levels - 1)
    wing = width // 2

    lane = np.arange(128) % (ROPE // 2)
    inverse = np.float32(rope_base) ** (-(2 * lane).astype(np.float32) / np.float32(ROPE))

    def turns(positions):
        phase = positions[:, None].astype(np.float64) * inverse[None, :].astype(np.float64)
        return np.concatenate([np.cos(phase), np.sin(phase)], 1).astype(np.float32)

    near_angle = turns(np.arange(count))
    if padded != mine:
        spread = np.pad(near_angle.reshape(tp_size, mine, 256), ((0, 0), (0, padded - mine), (0, 0)))
        near_angle = np.concatenate([near_angle, spread.reshape(queries, 256)], 0)
    far_angle = turns(np.arange(ep_size) * count)[:, None, :]

    def pad_rows(values):
        if padded == mine:
            return values
        values = values.reshape(tp_size, mine, values.shape[1])
        return jnp.pad(values, ((0, 0), (0, padded - mine), (0, 0))).reshape(queries, -1)

    dma = pltpu.SemaphoreType.DMA
    vmem = pl.BlockSpec(memory_space=pltpu.VMEM)
    far = pl.BlockSpec(memory_space=pl.ANY)
    small = (
        pad_rows(q_latent), kv_latent, rope_key.T, q_gain[None, :], kv_gain[None, :],
        jnp.asarray(near_angle), jnp.asarray(far_angle), expert_in, norm_gain[None, :], routes.T, route_scores.T,
    )
    mixed, expert_out = pl.pallas_call(
        functools.partial(layer_kernel, (ep_size, tp_size, slots, choose, heads, extent)),
        out_shape=(
            jax.ShapeDtypeStruct((padded, width), BF16),
            jax.ShapeDtypeStruct((tokens, features), BF16),
        ),
        in_specs=[far] * 18,
        out_specs=(far, far),
        scratch_shapes=[
            pltpu.VMEM((padded, width), BF16),
            pltpu.VMEM((tokens, features), BF16),
            *[pltpu.VMEM(value.shape, value.dtype) for value in small],
            pltpu.VMEM(w_query.shape, BF16),
            pltpu.VMEM(w_key.shape, BF16),
            pltpu.VMEM(w_value.shape, BF16),
            pltpu.VMEM(w_mix_out.shape, BF16),
            pltpu.VMEM((width, units), BF16),
            pltpu.VMEM((width, units), BF16),
            pltpu.VMEM((units, width), BF16),
            pltpu.VMEM((ep_size, 4, count // 4, kv_latent.shape[1]), BF16),
            pltpu.VMEM((ep_size, count // 2, 128), BF16),
            pltpu.VMEM((heads, ep_size * count, NOPE + 128), BF16),
            pltpu.VMEM((ep_size * count, heads * VDIM), BF16),
            pltpu.VMEM((heads, queries, NOPE + 128), BF16),
            pltpu.VMEM((queries, heads * VDIM), BF16),
            pltpu.VMEM((2, extent[1], extent[0], padded, wing), BF16),
            pltpu.VMEM((2, ahead, most, padded, wing), BF16),
            pltpu.VMEM((2, ahead, padded, wing), BF16),
            pltpu.VMEM((2, ahead, padded, wing), BF16),
            pltpu.VMEM((tokens, width), BF16),
            pltpu.VMEM((ep_size * slots, tokens), BF16),
            pltpu.VMEM((tokens, 128), F32),
            pltpu.VMEM((ep_size, slots, features), BF16),
            pltpu.VMEM((slots, width), BF16),
            pltpu.VMEM((ep_size, slots, width), BF16),
            pltpu.VMEM((2 * slots, units), BF16),
            pltpu.VMEM((ep_size, extent[1], extent[0], slots, features), BF16),
            pltpu.VMEM((ep_size, ahead, most, slots, features), BF16),
            pltpu.VMEM((ep_size, ahead, slots, features), BF16),
            pltpu.VMEM((ep_size, ahead, slots, features), BF16),
            pltpu.VMEM((ep_size, slots, features), BF16),
            pltpu.VMEM((ep_size, slots, features), BF16),
            dma((7,)), dma((11,)), dma((20,)),
            dma((away, 2)), dma((away, 2)), dma((away, 4)), dma((2,)),
            dma((away, 2)), dma((away, 2, max(1, tp_size - 1))), dma((1,)),
            dma((levels, 2, ahead)), dma((levels, 2, ahead)), dma((levels, 2)),
            dma((2, ahead)), dma((2, ahead)),
        ],
        compiler_params=pltpu.CompilerParams(
            collective_id=0, has_side_effects=True, vmem_limit_bytes=60 * 1024 * 1024
        ),
    )(
        *small,
        w_query, w_key, w_value, w_mix_out, w_gate[0], w_up[0], w_down[0],
    )
    return pl.pallas_call(
        hand_over,
        out_shape=(
            jax.ShapeDtypeStruct((mine, width), BF16),
            jax.ShapeDtypeStruct((tokens, features), BF16),
        ),
        in_specs=[vmem] * 2,
        out_specs=(vmem, vmem),
    )(mixed, expert_out)


def solution(mesh):
    in_specs = (
        P("ep", None),
        P("ep", None),
        P("ep", None),
        P(),
        P(),
        P(None, "tp"),
        P(None, "tp"),
        P(None, "tp"),
        P("tp", None),
        P("ep", None),
        P(),
        P("ep", None),
        P("ep", None),
        P("ep", None, "tp"),
        P("ep", None, "tp"),
        P("ep", "tp", None),
    )
    out_specs = (P(("ep", "tp"), None), P("ep", "tp"))
    return jax.shard_map(body, mesh=mesh, in_specs=in_specs, out_specs=out_specs, check_vma=False)
```
